32 devices in a mesh: ep: 4 (over y, x), tp: 8 (over z, core).
Axes of the slice: x: 2, y: 2, z: 4, core: 2. Of those that a mesh axis runs over, the one named last changes fastest.
Arguments:
- query_rows: bfloat16 [512, 2048], P('ep', 'tp'), may hold values from -32 to 32
- key_rows: bfloat16 [512, 2048], P('ep', 'tp'), may hold values from -8 to 8
- value_rows: bfloat16 [512, 2048], P('ep', 'tp'), may hold values from -8 to 8
- query_norm_gain: float32 [64], replicated, may hold values from 0.1 to 1.9
- key_gain: float32 [64], replicated, may hold values from 0.1 to 1.9
- break_offset: float32 [32], P('tp'), may hold values from -12 to 3
- mixer_out_weight: bfloat16 [2048, 2048], P('tp'), may hold values from -0.75 to 0.75
- routed_tokens: bfloat16 [4096, 2048], P(('ep', 'tp')), may hold values from -6 to 6
- expert_gain: float32 [2048], replicated, may hold values from 0.1 to 1.9
- routes: int32 [4096, 2], P(('ep', 'tp')), may hold values from 0 to 3, as said below
- route_scores: float32 [4096, 2], P(('ep', 'tp')), may hold values from -6 to 6
- gate_weight: bfloat16 [4, 2048, 3584], P('ep', None, 'tp'), may hold values from -0.125 to 0.125
- up_weight: bfloat16 [4, 2048, 3584], P('ep', None, 'tp'), may hold values from -0.125 to 0.125
- down_weight: bfloat16 [4, 3584, 2048], P('ep', 'tp'), may hold values from -0.09375 to 0.09375
Outputs:
- attention_output: bfloat16 [512, 2048], P(('ep', 'tp'))
- expert_output: bfloat16 [4096, 2048], P(('ep', 'tp'))
The draws below stay inside these ranges and needn't reach their ends.
Inputs may be any that keep to these rules, and one draw needn't show every extreme that they name: `routes`: each row names 2 different experts. Among the rows of one device no expert is named more than 64 times, and one expert is named exactly 64 times by the rows of every device.
All inputs are finite; a program needn't handle non-finite values.
Results may differ from the reference program's by a relative error of at most 0.018.
Values may be sent and summed in bfloat16 or wider, within the bound.
No kernel may reach another device: no remote copies, remote signals or barrier semaphores. Data moves between devices by JAX's collectives and lax.ppermute only.
A program may use at most 128 MiB of HBM per device.

```python
import math
import jax
import jax.numpy as jnp
from jax import lax

D = 2048
HEADS = 32
HEAD_DIM = 64
FFE = 3584
TOP_K = 2
TOK_DEV = 128
SEG = 128
SEQUENCE_TOKENS = 512
ROUTED = 4096
EXPERTS = 4
CAP = 64
N_TP = 8


def head_axes(key):
    sample = jax.random.normal(jax.random.fold_in(key, 101), (HEADS, HEAD_DIM), jnp.float32)
    return sample * lax.rsqrt(jnp.mean(sample * sample, axis=1, keepdims=True))


def draw_query_rows(key, part):
    direction = head_axes(key)
    jitter = jax.random.normal(jax.random.fold_in(key, 1), (SEQUENCE_TOKENS, HEADS, HEAD_DIM), jnp.float32)
    rows_out = jnp.clip(0.5 * jitter + direction[None], -32.0, 32.0)
    return rows_out.reshape(SEQUENCE_TOKENS, HEADS * HEAD_DIM).astype(jnp.bfloat16)


def draw_key_rows(key, part):
    direction = head_axes(key)
    blocks_count = SEQUENCE_TOKENS // SEG
    token_position = jnp.arange(SEQUENCE_TOKENS)
    jitter = jax.random.normal(jax.random.fold_in(key, 3), (SEQUENCE_TOKENS, HEADS, HEAD_DIM), jnp.float32)
    low_end = 0.4
    high_end = 1.6
    factor = jnp.exp(jax.random.uniform(jax.random.fold_in(key, 4), (blocks_count,), jnp.float32, jnp.log(low_end), jnp.log(high_end)))
    spread = jax.random.uniform(jax.random.fold_in(key, 5), (SEQUENCE_TOKENS, HEADS), jnp.float32, 0.6, 1.4)
    toward = -factor[token_position // SEG][:, None] * spread
    micro_batches = jax.random.randint(jax.random.fold_in(key, 6), (4,), 0, SEQUENCE_TOKENS)
    broken_stick = jnp.any(token_position[:, None] == micro_batches[None, :], axis=1)
    toward = jnp.where(broken_stick[:, None], 0.2, toward)
    rows_out = jnp.clip(0.5 * jitter + toward[:, :, None] * direction[None], -8.0, 8.0)
    return rows_out.reshape(SEQUENCE_TOKENS, HEADS * HEAD_DIM).astype(jnp.bfloat16)


def draw_value_rows(key, part):
    blocks_count = SEQUENCE_TOKENS // SEG
    levels = jax.random.uniform(jax.random.fold_in(key, 7), (blocks_count, HEADS * HEAD_DIM), jnp.float32, -1.5, 1.5)
    jitter = jax.random.normal(jax.random.fold_in(key, 8), (SEQUENCE_TOKENS, HEADS * HEAD_DIM), jnp.float32)
    rows_out = jnp.clip(jitter + jnp.repeat(levels, SEG, axis=0), -8.0, 8.0)
    return rows_out.astype(jnp.bfloat16)


def draw_break_offset(key, part):
    quick_share = 0.5
    quick = jax.random.uniform(jax.random.fold_in(key, 9), (HEADS,), jnp.float32) < quick_share
    quick_value = jax.random.uniform(jax.random.fold_in(key, 10), (HEADS,), jnp.float32, 2.0, 3.0)
    slow_value = jax.random.uniform(jax.random.fold_in(key, 11), (HEADS,), jnp.float32, 5.0, 6.0) - jnp.log(SEQUENCE_TOKENS * 1.0)
    return jnp.where(quick, quick_value, slow_value).astype(jnp.float32)


def draw_routes(key, part):
    blocks_count = ROUTED // TOK_DEV

    def one_block(block_key):
        reserve = jnp.tile(jnp.arange(1, EXPERTS, dtype=jnp.int32), CAP)
        reserve = jax.random.permutation(jax.random.fold_in(block_key, 1), reserve)
        remainder = jnp.sort(reserve[:TOK_DEV * TOP_K - CAP])
        ordered = jnp.concatenate([jnp.zeros((CAP,), jnp.int32), remainder])
        paired = ordered.reshape(TOP_K, TOK_DEV).T
        shuffle = jax.random.permutation(jax.random.fold_in(block_key, 2), TOK_DEV)
        labels = jax.random.permutation(jax.random.fold_in(block_key, 3), EXPERTS).astype(jnp.int32)
        return labels[paired[shuffle]]
    block_keys = jax.random.split(jax.random.fold_in(key, 13), blocks_count)
    chosen = jax.vmap(one_block)(block_keys).reshape(ROUTED, TOP_K)
    return chosen.astype(jnp.int32)


def block_scale(rng, extent, shards, low, largest):
    factor_of, own = 1.0, jax.random.fold_in(rng, 6)
    for position, parts in shards:
        heights = jnp.exp(jax.random.uniform(jax.random.fold_in(own, position), (parts,), jnp.float32, low / len(shards), largest / len(shards)))
        factor_of = factor_of * jnp.repeat(heights, extent[position] // parts).reshape([-1 if axis == position else 1 for axis in range(len(extent))])
    return factor_of


def noise(rng, dims, deviation, reach, cuts=(), held_as=jnp.bfloat16):
    values = jax.random.normal(rng, dims, jnp.float32) * deviation
    if len(cuts) > 0:
        values = block_scale(rng, dims, cuts, -0.22, 0.18) * values
    return jnp.clip(values, min=-reach, max=reach).astype(held_as)


def setup_inputs(seed: int = 0) -> dict:
    key_list = jax.random.split(jax.random.key(seed), 15)
    return {
        "query_rows": draw_query_rows(jax.random.fold_in(key_list[14], 71), 0),
        "key_rows": draw_key_rows(jax.random.fold_in(key_list[14], 71), 0),
        "value_rows": draw_value_rows(jax.random.fold_in(key_list[14], 71), 0),
        "query_norm_gain": jnp.clip(1.0 + 0.18 * jax.random.normal(key_list[3], (HEAD_DIM,), jnp.float32), 0.1, 1.9),
        "key_gain": jnp.clip(1.0 + 0.18 * jax.random.normal(key_list[4], (HEAD_DIM,), jnp.float32), 0.1, 1.9),
        "break_offset": draw_break_offset(jax.random.fold_in(key_list[14], 71), 0),
        "mixer_out_weight": noise(key_list[6], (HEADS * HEAD_DIM, D), HEAD_DIM ** -0.5, 0.75, ((0, 8),)),
        "routed_tokens": noise(key_list[7], (ROUTED, D), 1.0, 6.0, ((0, 32),)),
        "expert_gain": jnp.clip(1.0 + 0.18 * jax.random.normal(key_list[8], (D,), jnp.float32), 0.1, 1.9),
        "routes": draw_routes(jax.random.fold_in(key_list[14], 71), 0),
        "route_scores": noise(key_list[10], (ROUTED, TOP_K), 1.5, 6.0, ((0, 32),), jnp.float32),
        "gate_weight": noise(key_list[11], (EXPERTS, D, FFE), D ** -0.5, 0.125, ((0, 4), (2, 8))),
        "up_weight": noise(key_list[12], (EXPERTS, D, FFE), D ** -0.5, 0.125, ((0, 4), (2, 8))),
        "down_weight": noise(key_list[13], (EXPERTS, FFE, D), FFE ** -0.5, 0.09375, ((0, 4), (1, 8))),
    }


EPS = 1e-06

def norm_heads(flat, gain):
    count = flat.shape[0]
    split = flat.astype(jnp.float32).reshape(count, -1, HEAD_DIM)
    scaled = split * lax.rsqrt(lax.optimization_barrier(jnp.mean(split * split, axis=2, keepdims=True)) + EPS)
    return (scaled * gain).astype(jnp.bfloat16)

def attention_part(query_rows, key_rows, value_rows, query_norm_gain, key_gain, break_offset, mixer_out_weight):
    length = query_rows.shape[0]
    query_norm = norm_heads(query_rows, query_norm_gain)
    key_norm = norm_heads(key_rows, key_gain)
    value_heads = value_rows.reshape(length, HEADS, HEAD_DIM)
    block_size = math.gcd(512, length)
    gathered = []
    for block_start in range(0, length, block_size):
        block_end = block_start + block_size
        query_place = block_start + jnp.arange(block_size, dtype=jnp.int32)[:, None]
        key_place = jnp.arange(block_end, dtype=jnp.int32)[None, :]
        before = key_place < query_place

        def one_head(inputs):
            query_head, key_head, value_head, offset_value = inputs
            scores = jnp.dot(query_head, key_head.T, preferred_element_type=jnp.float32) * HEAD_DIM ** (-0.5) + offset_value
            log_rise = jax.nn.log_sigmoid(scores)
            log_fail = jnp.where(before, log_rise - scores, 0.0)
            log_after = lax.cumsum(log_fail, axis=1, reverse=True) - log_fail
            weights = jnp.where(before, jnp.exp(log_rise + log_after), 0.0).astype(jnp.bfloat16)
            return jnp.dot(weights, value_head, preferred_element_type=jnp.float32).astype(jnp.bfloat16)
        heads_out = lax.map(one_head, (jnp.moveaxis(query_norm[block_start:block_end], 1, 0), jnp.moveaxis(key_norm[:block_end], 1, 0), jnp.moveaxis(value_heads[:block_end], 1, 0), break_offset))
        gathered.append(jnp.moveaxis(heads_out, 0, 1).reshape(block_size, HEADS * HEAD_DIM))
    heads_mixed = jnp.concatenate(gathered, axis=0)
    group_width = HEADS * HEAD_DIM // N_TP
    running_sum = jnp.zeros((length, D), jnp.float32)
    for group_index in range(N_TP):
        low_edge = group_index * group_width
        term = jnp.dot(heads_mixed[:, low_edge:low_edge + group_width], mixer_out_weight[low_edge:low_edge + group_width], preferred_element_type=jnp.float32).astype(jnp.bfloat16)
        running_sum = running_sum + term.astype(jnp.float32)
    return running_sum.astype(jnp.bfloat16)

def expert_part(routed_tokens, expert_gain, routes, route_scores, gate_weight, up_weight, down_weight):
    row_count = routed_tokens.shape[0]
    as_float = routed_tokens.astype(jnp.float32)
    normed = (as_float * lax.rsqrt(lax.optimization_barrier(jnp.mean(as_float * as_float, axis=1, keepdims=True)) + EPS) * expert_gain).astype(jnp.bfloat16)
    differences = route_scores[:, None, :] - route_scores[:, :, None]
    route_weight = 1.0 / lax.optimization_barrier(jnp.sum(jnp.exp(differences), axis=2))
    flat_routes = routes.reshape(-1).astype(jnp.int32)
    copy_count = flat_routes.shape[0]
    block_count = row_count // TOK_DEV
    member = (flat_routes[:, None] == jnp.arange(EXPERTS, dtype=jnp.int32)[None, :]).astype(jnp.int32)
    member = member.reshape(block_count, TOK_DEV * TOP_K, EXPERTS)
    ahead = lax.optimization_barrier(jnp.sum((jnp.cumsum(member, axis=1) - member) * member, axis=2)).reshape(-1)
    owner = jnp.arange(copy_count, dtype=jnp.int32) // (TOK_DEV * TOP_K)
    slot_index = (owner * CAP + ahead).astype(jnp.int32)
    sources = jnp.repeat(normed, TOP_K, axis=0)
    room = block_count * CAP
    unit_width = FFE // N_TP

    def single_expert(carry, expert_index):
        chosen = flat_routes == expert_index
        target = jnp.where(chosen, slot_index, room).astype(jnp.int32)
        rows_in = jnp.zeros((room, D), jnp.bfloat16).at[target].set(sources, mode='drop')
        gate_part = jnp.dot(rows_in, gate_weight[expert_index], preferred_element_type=jnp.float32)
        up_part = jnp.dot(rows_in, up_weight[expert_index], preferred_element_type=jnp.float32)
        hidden = (jax.nn.silu(gate_part) * up_part).astype(jnp.bfloat16)
        down_here = down_weight[expert_index]
        running_sum = jnp.zeros((room, D), jnp.float32)
        for unit_index in range(N_TP):
            low_edge = unit_index * unit_width
            term = jnp.dot(hidden[:, low_edge:low_edge + unit_width], down_here[low_edge:low_edge + unit_width], preferred_element_type=jnp.float32).astype(jnp.bfloat16)
            running_sum = running_sum + term.astype(jnp.float32)
        result = running_sum.astype(jnp.bfloat16)
        picked = result[jnp.minimum(target, room - 1)]
        return (jnp.where(chosen[:, None], picked.astype(jnp.float32), carry), None)
    results, _ = lax.scan(single_expert, jnp.zeros((copy_count, D), jnp.float32), jnp.arange(EXPERTS, dtype=jnp.int32))
    results = results.reshape(row_count, TOP_K, D)
    return lax.optimization_barrier(jnp.sum(route_weight[..., None] * results, axis=1)).astype(jnp.bfloat16)

def reference(query_rows, key_rows, value_rows, query_norm_gain, key_gain, break_offset, mixer_out_weight, routed_tokens, expert_gain, routes, route_scores, gate_weight, up_weight, down_weight):
    attention_output = attention_part(query_rows, key_rows, value_rows, query_norm_gain, key_gain, break_offset, mixer_out_weight)
    expert_output = expert_part(routed_tokens, expert_gain, routes, route_scores, gate_weight, up_weight, down_weight)
    return (attention_output, expert_output)
```

```python
import jax
import jax.numpy as jnp
from jax import lax
from jax.sharding import PartitionSpec as P

HEAD_DIM = 64
TOP_K = 2
CORES = 2
LANES = 128


EPS = 1e-06


def partner(index, step, count):
    if count & (count - 1) == 0:
        return index ^ step
    return (index + step) % count


def relative(target, index, count):
    if count & (count - 1) == 0:
        return target ^ index
    return (target - index) % count


def over_ep(array, step, back=False):
    count = lax.axis_size("ep")
    pairs = [(i, partner(i, step, count)) for i in range(count)]
    if back:
        pairs = [(b, a) for a, b in pairs]
    return lax.ppermute(array, "ep", pairs)


def over_z(array, step, back=False):
    count = lax.axis_size("tp") // CORES
    pairs = [
        (i * CORES + c, partner(i, step, count) * CORES + c)
        for i in range(count)
        for c in range(CORES)
    ]
    if back:
        pairs = [(b, a) for a, b in pairs]
    return lax.ppermute(array, "tp", pairs)


def over_core(array, step):
    count = lax.axis_size("tp")
    pairs = [(i, i // CORES * CORES + (i + step) % CORES) for i in range(count)]
    return lax.ppermute(array, "tp", pairs)


def norm_heads(flat, gain):
    count = flat.shape[0]
    split = flat.astype(jnp.float32).reshape(count, -1, HEAD_DIM)
    scaled = split * lax.rsqrt(jnp.mean(split * split, axis=2, keepdims=True) + EPS)
    return (scaled * gain).astype(jnp.bfloat16)


def attention(query_rows, key_rows, value_rows, query_norm_gain, key_gain, break_offset):
    row_count = query_rows.shape[0]
    query_norm = norm_heads(query_rows, query_norm_gain)
    key_flat = norm_heads(key_rows, key_gain).reshape(row_count, -1)
    width = key_flat.shape[1]
    both = jnp.concatenate([key_flat, value_rows], axis=1)
    both = lax.all_gather(both, "ep", axis=0, tiled=True)
    key_count = both.shape[0]
    key_norm = both[:, :width].reshape(key_count, -1, HEAD_DIM)
    value_heads = both[:, width:].reshape(key_count, -1, HEAD_DIM)
    query_place = lax.axis_index("ep") * row_count + jnp.arange(row_count)
    key_place = jnp.arange(key_count)
    before = (key_place[None, :] < query_place[:, None])[None]
    scores = jnp.einsum("qhd,khd->hqk", query_norm, key_norm, preferred_element_type=jnp.float32)
    scores = scores * HEAD_DIM ** (-0.5) + break_offset[:, None, None]
    log_rise = jax.nn.log_sigmoid(scores)
    log_fail = jnp.where(before, log_rise - scores, 0.0)
    later = (key_place[:, None] > key_place[None, :]).astype(jnp.float32)
    log_after = jnp.einsum(
        "hqj,jk->hqk",
        log_fail,
        later,
        precision=lax.Precision.HIGHEST,
        preferred_element_type=jnp.float32,
    )
    weights = jnp.where(before, jnp.exp(log_rise + log_after), 0.0).astype(jnp.bfloat16)
    mixed = jnp.einsum("hqk,khd->qhd", weights, value_heads, preferred_element_type=jnp.float32)
    return mixed.astype(jnp.bfloat16).reshape(row_count, -1)


def mixer_reduce(heads_mixed, mixer_out_weight):
    terms = jnp.dot(heads_mixed, mixer_out_weight, preferred_element_type=jnp.float32).astype(
        jnp.bfloat16
    )
    count = lax.axis_size("tp")
    terms = lax.all_to_all(terms, "tp", split_axis=0, concat_axis=0, tiled=True)
    terms = terms.reshape(count, -1, terms.shape[1])
    return jnp.sum(terms.astype(jnp.float32), axis=0).astype(jnp.bfloat16)


def route_columns(routes, route_scores, expert_count, capacity):
    token_count = routes.shape[0]
    experts = jnp.arange(expert_count, dtype=jnp.int32)[None, :]
    member = [(routes[:, k : k + 1] == experts).astype(jnp.float32) for k in range(TOP_K)]
    place = jnp.arange(token_count)
    earlier = (place[None, :] < place[:, None]).astype(jnp.float32)
    columns = []
    taken = jnp.zeros((1, expert_count), jnp.float32)
    for k in range(TOP_K):
        ahead = jnp.dot(earlier, member[k], preferred_element_type=jnp.float32) + taken
        columns.append(jnp.sum(member[k] * ahead, axis=1, keepdims=True))
        taken = taken + jnp.sum(member[k], axis=0, keepdims=True)
    me = lax.axis_index("ep")
    columns.append(relative(routes, me, expert_count).astype(jnp.float32))
    differences = route_scores[:, None, :] - route_scores[:, :, None]
    columns.append(1.0 / jnp.sum(jnp.exp(differences), axis=2))
    packed = jnp.concatenate(columns, axis=1)
    return jnp.pad(packed, ((0, 0), (0, LANES - packed.shape[1]))).astype(jnp.bfloat16)


def choose(columns, slot_count, capacity):
    columns = columns.astype(jnp.float32)
    slots = jnp.arange(slot_count, dtype=jnp.float32)[None, :]
    picked = 0.0
    weighted = 0.0
    for k in range(TOP_K):
        ahead = columns[:, k : k + 1]
        near = columns[:, TOP_K + k : TOP_K + k + 1]
        weight = columns[:, 2 * TOP_K + k : 2 * TOP_K + k + 1]
        hit = near * capacity + ahead == slots
        picked = picked + jnp.where(hit, 1.0, 0.0)
        weighted = weighted + jnp.where(hit, weight, 0.0)
    return picked.astype(jnp.bfloat16), weighted.astype(jnp.bfloat16)


def expert_layer(rows, weights):
    total = 0.0
    for gate, up, down in weights:
        gate_piece = jnp.dot(rows, gate, preferred_element_type=jnp.float32)
        up_piece = jnp.dot(rows, up, preferred_element_type=jnp.float32)
        hidden = (jax.nn.silu(gate_piece) * up_piece).astype(jnp.bfloat16)
        total = total + jnp.dot(hidden, down, preferred_element_type=jnp.float32)
    return total.astype(jnp.bfloat16)


def body(
    query_rows,
    key_rows,
    value_rows,
    query_norm_gain,
    key_gain,
    break_offset,
    mixer_out_weight,
    routed_tokens,
    expert_gain,
    routes,
    route_scores,
    gate_weight,
    up_weight,
    down_weight,
):
    expert_count = lax.axis_size("ep")
    levels = lax.axis_size("tp") // CORES
    token_count = routed_tokens.shape[0]
    model_width = routed_tokens.shape[1]
    capacity = max(2, token_count * TOP_K // expert_count)
    slot_count = expert_count * capacity

    as_float = routed_tokens.astype(jnp.float32)
    normed = (
        as_float
        * lax.rsqrt(jnp.mean(as_float * as_float, axis=1, keepdims=True) + EPS)
        * expert_gain
    ).astype(jnp.bfloat16)
    columns = route_columns(routes, route_scores, expert_count, capacity)
    packed = jnp.concatenate([normed, columns], axis=1)
    blocks = [packed] + [over_z(packed, step) for step in range(1, levels)]

    own = (gate_weight[0], up_weight[0], down_weight[0])
    weights = [own] + [tuple(over_core(w, step) for w in own) for step in range(1, CORES)]

    arrived = []
    mixes = []
    for block in blocks:
        picked, weighted = choose(block[:, model_width:], slot_count, capacity)
        mixes.append(weighted)
        outgoing = jnp.einsum(
            "ts,td->sd", picked, block[:, :model_width], preferred_element_type=jnp.float32
        ).astype(jnp.bfloat16)
        pieces = [outgoing[e * capacity : (e + 1) * capacity] for e in range(expert_count)]
        arrived.append(
            [pieces[0]] + [over_ep(pieces[step], step) for step in range(1, expert_count)]
        )

    heads_mixed = attention(
        query_rows, key_rows, value_rows, query_norm_gain, key_gain, break_offset
    )
    mixer_sum = mixer_reduce(heads_mixed, mixer_out_weight)

    total = 0.0
    for level in range(levels):
        rows = jnp.concatenate(arrived[level], axis=0)
        results = expert_layer(rows, weights)
        pieces = [results[e * capacity : (e + 1) * capacity] for e in range(expert_count)]
        returned = [pieces[0]] + [
            over_ep(pieces[step], step, back=True) for step in range(1, expert_count)
        ]
        share = jnp.dot(
            mixes[level], jnp.concatenate(returned, axis=0), preferred_element_type=jnp.float32
        )
        if level > 0:
            share = over_z(share.astype(jnp.bfloat16), level, back=True).astype(jnp.float32)
        total = total + share
    return (mixer_sum, total.astype(jnp.bfloat16))


def solution(mesh):
    in_specs = (
        P("ep", "tp"),
        P("ep", "tp"),
        P("ep", "tp"),
        P(),
        P(),
        P("tp"),
        P("tp", None),
        P(("ep", "tp"), None),
        P(),
        P(("ep", "tp"), None),
        P(("ep", "tp"), None),
        P("ep", None, "tp"),
        P("ep", None, "tp"),
        P("ep", "tp", None),
    )
    out_specs = (P(("ep", "tp"), None), P(("ep", "tp"), None))
    return jax.shard_map(body, mesh=mesh, in_specs=in_specs, out_specs=out_specs, check_vma=False)
```

```python
import jax
import jax.numpy as jnp
from jax import lax
from jax.experimental import pallas as pl
from jax.experimental.pallas import tpu as pltpu
from jax.sharding import PartitionSpec as P


HEAD_DIM = 64
TOP_K = 2
CORES = 2
LANES = 128
MOST_PERMUTES = 8


EPS = 1e-06


def partner(index, step, count):
    if count & (count - 1) == 0:
        return index ^ step
    return (index + step) % count


def relative(target, index, count):
    if count & (count - 1) == 0:
        return target ^ index
    return (target - index + count) % count


def over_ep(pieces, back=False):
    count = lax.axis_size("ep")
    if len(pieces) == 1:
        return [lax.all_to_all(pieces[0], "ep", split_axis=0, concat_axis=0, tiled=True)]
    moved = [pieces[0]]
    for step in range(1, count):
        pairs = [(i, partner(i, step, count)) for i in range(count)]
        if back:
            pairs = [(b, a) for a, b in pairs]
        moved.append(lax.ppermute(pieces[step], "ep", pairs))
    return moved


def over_z(array, pairs):
    pairs = [(a * CORES + c, b * CORES + c) for a, b in pairs for c in range(CORES)]
    return lax.ppermute(array, "tp", pairs)


RELAYED = 4


def gather_z(packed, levels):
    if levels != RELAYED:
        return [
            [over_z(packed, [(i, partner(i, step, levels)) for i in range(levels)])]
            for step in range(1, levels)
        ]
    beside = over_z(packed, [(0, 1), (1, 0), (2, 3), (3, 2)])
    across = over_z(packed, [(1, 2), (2, 1)])
    beyond = over_z(beside, [(1, 2), (2, 1)])
    second = over_z(across, [(1, 0), (2, 3)])
    third = over_z(beyond, [(1, 0), (2, 3)])
    return [[beside], [second, across], [third, beyond]]


def target_level(index, outer, level, levels):
    if levels != RELAYED:
        if levels & (levels - 1) == 0:
            return index ^ level
        return (index - level + levels) % levels
    return index ^ (3 - outer) if level == 2 else index ^ (2 + outer)


def over_core(array, step):
    count = lax.axis_size("tp")
    pairs = [(i, i // CORES * CORES + (i + step) % CORES) for i in range(count)]
    return lax.ppermute(array, "tp", pairs)


def dot(a, b, dims=((1,), (0,)), precision=None):
    return lax.dot_general(
        a, b, (dims, ((), ())), precision=precision, preferred_element_type=jnp.float32
    )


def whole(array):
    return pl.BlockSpec(array.shape, lambda *_: (0,) * array.ndim)


VECTOR = pl.BlockSpec(memory_space=pltpu.VMEM)
REMAIN = pl.BlockSpec(memory_space=pltpu.HBM)
PARAMS = pltpu.CompilerParams(vmem_limit_bytes=16 * 1024 * 1024)


SCALAR = pl.BlockSpec(memory_space=pltpu.SMEM)


def head_norm(rows, gain):
    split = rows.astype(jnp.float32)
    mean = jnp.sum(split * split, axis=1, keepdims=True) * (1.0 / HEAD_DIM)
    return (split * lax.rsqrt(mean + EPS) * gain).astype(jnp.bfloat16)


def attention_kernel(slots, *refs):
    me_ref, offset_ref, query_ref, query_gain_ref, key_gain_ref, mixer_ref = refs[:6]
    key_ref, value_ref, *block_refs, keep_ref, give_ref, terms_ref = refs[6:]
    row_count, width = query_ref.shape
    head_count = width // HEAD_DIM
    me = me_ref[0]
    if slots is None:
        blocks = [(block_refs[0][:, :width], block_refs[0][:, width:])]
        places = [0]
    else:
        fold = block_refs[0].shape[1] // (2 * width)
        part = row_count // fold
        blocks = [(key_ref[...], value_ref[...])]
        for ref in block_refs:
            rows = ref[slots : slots + part]
            rows = jnp.concatenate(
                [rows[:, 2 * width * f : 2 * width * (f + 1)] for f in range(fold)], axis=0
            )
            blocks.append((rows[:, :width], rows[:, width:]))
        places = [partner(me, step, len(blocks)) * row_count for step in range(len(blocks))]
    query_place = me * row_count + lax.broadcasted_iota(jnp.int32, (row_count, 1), 0)
    block_rows = blocks[0][0].shape[0]
    row = lax.broadcasted_iota(jnp.int32, (block_rows, block_rows), 0)
    column = lax.broadcasted_iota(jnp.int32, (block_rows, block_rows), 1)
    later = jnp.where(row > column, 1.0, 0.0).astype(jnp.bfloat16)
    key_iota = lax.broadcasted_iota(jnp.int32, (1, block_rows), 1)
    mixed = []
    for head in range(head_count):
        cut = slice(head * HEAD_DIM, (head + 1) * HEAD_DIM)
        query = head_norm(query_ref[:, cut], query_gain_ref[...])
        rises, fails, totals, allows = [], [], [], []
        for index, (keys, _) in enumerate(blocks):
            key = head_norm(keys[:, cut], key_gain_ref[...])
            scores = dot(query, key, ((1,), (1,))) * HEAD_DIM ** (-0.5) + offset_ref[head]
            before = places[index] + key_iota < query_place
            rise = jnp.minimum(scores, 0.0) - jnp.log1p(jnp.exp(-jnp.abs(scores)))
            fail = jnp.where(before, rise - scores, 0.0)
            rises.append(rise)
            fails.append(fail)
            allows.append(before)
            totals.append(jnp.sum(fail, axis=1, keepdims=True))
        mix = jnp.zeros((row_count, HEAD_DIM), jnp.float32)
        for index, (_, values) in enumerate(blocks):
            after = jnp.zeros((row_count, 1), jnp.float32)
            for other in range(len(blocks)):
                if other != index:
                    behind = places[other] > places[index]
                    after = after + jnp.where(behind, totals[other], 0.0)
            rest = fails[index]
            for _ in range(3):
                part = rest.astype(jnp.bfloat16)
                after = after + dot(part, later)
                rest = rest - part.astype(jnp.float32)
            weights = jnp.where(allows[index], jnp.exp(rises[index] + after), 0.0)
            mix = mix + dot(weights.astype(jnp.bfloat16), values[:, cut])
        mixed.append(mix.astype(jnp.bfloat16))
    terms = dot(jnp.concatenate(mixed, axis=1), mixer_ref[...]).astype(jnp.bfloat16)
    levels, owned = keep_ref.shape[:2]
    for index in range(levels * CORES):
        terms_ref[index] = terms[index * owned : (index + 1) * owned]
    core = me_ref[2]
    for level in range(levels):
        keep_ref[level] = terms_ref[level * CORES + core]
        give_ref[level] = terms_ref[level * CORES + 1 - core]


def attention(
    me, blocks, slots, query_rows, key_rows, value_rows, query_norm_gain, key_gain, offset, mixer
):
    row_count = query_rows.shape[0]
    owners = lax.axis_size("tp")
    shape = (owners // CORES, row_count // owners, mixer.shape[1])
    args = (query_rows, query_norm_gain[None], key_gain[None], mixer, key_rows, value_rows)
    return pl.pallas_call(
        lambda *refs: attention_kernel(slots, *refs),
        out_shape=[jax.ShapeDtypeStruct(shape, jnp.bfloat16)] * 2,
        grid=(1,),
        in_specs=[SCALAR, SCALAR] + [whole(a) for a in (*args, *blocks)],
        out_specs=[VECTOR] * 2,
        scratch_shapes=[pltpu.VMEM((owners, *shape[1:]), jnp.bfloat16)],
        compiler_params=PARAMS,
        cost_estimate=pl.CostEstimate(
            flops=6_000_000_000, bytes_accessed=3_000_000, transcendentals=1_000_000
        ),
        name="attention",
    )(me, offset, *args, *blocks)


def hits(rows, slot_count, capacity):
    slots = lax.broadcasted_iota(jnp.int32, (slot_count, 1), 0).astype(jnp.float32)
    return [
        rows[TOP_K + k : TOP_K + k + 1] * capacity + rows[k : k + 1] == slots for k in range(TOP_K)
    ]


def spread(rows, tokens, out_refs, slot_count, capacity):
    piece_rows = slot_count // len(out_refs)
    picked = 0.0
    for hit in hits(rows, slot_count, capacity):
        picked = picked + jnp.where(hit, 1.0, 0.0)
    picked = picked.astype(jnp.bfloat16)
    for index, ref in enumerate(out_refs):
        part = picked[index * piece_rows : (index + 1) * piece_rows]
        ref[:piece_rows] = dot(part, tokens).astype(jnp.bfloat16)


def prepare_kernel(expert_count, capacity, me_ref, *refs):
    inputs, outputs, scratch = refs[:6], refs[6:-6], refs[-6:]
    packed_ref, *out_refs = outputs
    both_ref = scratch[4]
    tokens_ref, gain_ref, routes_ref, scores_ref = scratch[:4]
    half = both_ref.shape[1] // 2
    targets = (*scratch[:4], both_ref.at[:, :half], both_ref.at[:, half:])
    copies = [
        pltpu.make_async_copy(source, target, scratch[5].at[index])
        for index, (source, target) in enumerate(zip(inputs, targets))
    ]
    for copy in copies:
        copy.start()
    for copy in copies:
        copy.wait()
    token_count, width = tokens_ref.shape
    as_float = tokens_ref[...].astype(jnp.float32)
    mean = jnp.sum(as_float * as_float, axis=1, keepdims=True) * (1.0 / width)
    normed = (as_float * lax.rsqrt(mean + EPS) * gain_ref[...]).astype(jnp.bfloat16)
    packed_ref[:, :width] = normed
    routes = routes_ref[...]
    scores = scores_ref[...]
    experts = lax.broadcasted_iota(jnp.int32, (expert_count, 1), 0)
    row = lax.broadcasted_iota(jnp.int32, (token_count, token_count), 0)
    column = lax.broadcasted_iota(jnp.int32, (token_count, token_count), 1)
    earlier = jnp.where(row < column, 1.0, 0.0).astype(jnp.bfloat16)
    taken = jnp.zeros((expert_count, 1), jnp.float32)
    aheads, nears, weights = [], [], []
    for k in range(TOP_K):
        chosen = routes[k : k + 1]
        member = jnp.where(chosen == experts, 1.0, 0.0)
        ahead = dot(member.astype(jnp.bfloat16), earlier) + taken
        aheads.append(jnp.sum(member * ahead, axis=0, keepdims=True))
        taken = taken + jnp.sum(member, axis=1, keepdims=True)
        if len(out_refs) == 1:
            near = chosen
        else:
            near = relative(chosen, me_ref[0], expert_count)
        nears.append(near.astype(jnp.float32))
        total = 0.0
        for j in range(TOP_K):
            total = total + jnp.exp(scores[j : j + 1] - scores[k : k + 1])
        weights.append(1.0 / total)
    rows = aheads + nears + weights
    rows = jnp.concatenate(
        rows + [jnp.zeros((LANES - len(rows), token_count), jnp.float32)], axis=0
    )
    packed_ref[:, width:] = rows.T.astype(jnp.bfloat16)
    slot_count = expert_count * capacity
    spread(rows, normed, out_refs, slot_count, capacity)
    for ref in out_refs[1:]:
        fold = width // both_ref.shape[1]
        part = both_ref.shape[0] // fold
        for f in range(fold):
            columns = slice(f * both_ref.shape[1], (f + 1) * both_ref.shape[1])
            ref[capacity:, columns] = both_ref[f * part : (f + 1) * part]


def piece_shapes(count, slot_count, width):
    return [
        jax.ShapeDtypeStruct((slot_count // count, width), jnp.bfloat16) for _ in range(count)
    ]


def prepare(me, tokens, gain, routes, scores, keys, values, expert_count, piece_count, capacity):
    token_count, width = tokens.shape
    both = (keys.shape[0], keys.shape[1] + values.shape[1])
    shapes = [jax.ShapeDtypeStruct((token_count, width + LANES), jnp.bfloat16)]
    shapes += piece_shapes(piece_count, expert_count * capacity, width)
    extra = both[0] * both[1] // width
    shapes[2:] = [jax.ShapeDtypeStruct((capacity + extra, width), jnp.bfloat16)] * (piece_count - 1)
    args = (tokens, gain[None], routes.T, scores.T, keys, values)
    args = tuple(pltpu.with_memory_space_constraint(a, pltpu.HBM) for a in args)
    packed, *pieces = pl.pallas_call(
        lambda *refs: prepare_kernel(expert_count, capacity, *refs),
        out_shape=shapes,
        in_specs=[SCALAR] + [REMAIN] * len(args),
        out_specs=[VECTOR] * len(shapes),
        scratch_shapes=[pltpu.VMEM(a.shape, a.dtype) for a in args[:4]]
        + [pltpu.VMEM(both, keys.dtype), pltpu.SemaphoreType.DMA((len(args),))],
        compiler_params=PARAMS,
        cost_estimate=pl.CostEstimate(
            flops=2_000_000_000, bytes_accessed=3_000_000, transcendentals=0
        ),
        name="prepare",
    )(me, *args)
    return packed, pieces


def select(me, candidates, piece_count, slot_count, capacity):
    token_count, width = candidates[0].shape
    width -= LANES

    def kernel(me_ref, *refs):
        packed = refs[0][...]
        if len(candidates) > 1:
            packed = jnp.where(me_ref[1] == 1, packed, refs[1][...])
        columns_ref, *out_refs = refs[len(candidates) :]
        columns_ref[...] = packed[:, width:]
        rows = packed[:, width:].astype(jnp.float32).T
        spread(rows, packed[:, :width], out_refs, slot_count, capacity)

    shapes = [jax.ShapeDtypeStruct((token_count, LANES), jnp.bfloat16)]
    shapes += piece_shapes(piece_count, slot_count, width)
    columns, *pieces = pl.pallas_call(
        kernel,
        out_shape=shapes,
        in_specs=[SCALAR] + [VECTOR] * len(candidates),
        out_specs=[VECTOR] * len(shapes),
        compiler_params=PARAMS,
        cost_estimate=pl.CostEstimate(
            flops=1_500_000_000, bytes_accessed=2_000_000, transcendentals=0
        ),
        name="select",
    )(me, *candidates)
    return columns, pieces


def expert_layer(pieces, piece_rows, weights, joined=False, addend=None):
    width = pieces[0].shape[1]
    count = len(pieces)
    row_count = count * piece_rows
    units = weights[0][0].shape[0]
    groups = len(weights)
    addends = [] if addend is None else [addend]
    far = [w for group in weights[1:] for w in group]

    def kernel(*refs):
        refs = list(refs)
        rows_refs = [refs.pop(0) for _ in pieces]
        addend_refs = [refs.pop(0) for _ in addends]
        own_refs = [refs.pop(0) for _ in range(3)]
        far_refs = [refs.pop(0) for _ in far]
        semaphores = refs.pop()
        near_refs = refs[len(refs) - len(far) :]
        out_refs = refs[: len(refs) - len(far)]
        copies = [
            pltpu.make_async_copy(source, target, semaphores.at[index])
            for index, (source, target) in enumerate(zip(far_refs, near_refs))
        ]
        for copy in copies:
            copy.start()
        rows = jnp.concatenate([ref[:piece_rows] for ref in rows_refs], axis=0)
        total = jnp.zeros((row_count, width), jnp.float32)
        for ref in addend_refs:
            total = ref[...].astype(jnp.float32)
        for g in range(groups):
            if g == 0:
                gate_ref, up_ref, down_ref = own_refs
            else:
                gate_ref, up_ref, down_ref = near_refs[3 * g - 3 : 3 * g]
                for copy in copies[3 * g - 3 : 3 * g]:
                    copy.wait()
            gate = dot(rows, gate_ref[...], ((1,), (1,)))
            up = dot(rows, up_ref[...], ((1,), (1,)))
            hidden = (gate / (1.0 + jnp.exp(-gate)) * up).astype(jnp.bfloat16)
            total = total + dot(hidden, down_ref[...])
        total = total.astype(jnp.bfloat16)
        part = row_count // len(out_refs)
        for index, ref in enumerate(out_refs):
            ref[...] = total[index * part : (index + 1) * part]

    shapes = piece_shapes(1 if joined else count, row_count, width)
    return list(
        pl.pallas_call(
            kernel,
            out_shape=shapes,
            in_specs=[VECTOR] * (count + len(addends) + 3) + [REMAIN] * len(far),
            out_specs=[VECTOR] * len(shapes),
            scratch_shapes=[pltpu.VMEM(w.shape, w.dtype) for w in far]
            + [pltpu.SemaphoreType.DMA((len(far),))],
            compiler_params=PARAMS,
            cost_estimate=pl.CostEstimate(
                flops=6 * row_count * units * groups * width,
                bytes_accessed=6 * units * groups * width,
                transcendentals=row_count * units * groups,
            ),
            name="expert_layer",
        )(*pieces, *addends, *weights[0], *far)
    )


def mixing(columns, piece_refs, capacity):
    slot_count = sum(ref.shape[0] for ref in piece_refs)
    columns = columns.astype(jnp.float32)
    slots = lax.broadcasted_iota(jnp.int32, (1, slot_count), 1).astype(jnp.float32)
    mix = 0.0
    for k in range(TOP_K):
        near = columns[:, TOP_K + k : TOP_K + k + 1]
        hit = near * capacity + columns[:, k : k + 1] == slots
        mix = mix + jnp.where(hit, columns[:, 2 * TOP_K + k : 2 * TOP_K + k + 1], 0.0)
    rows = jnp.concatenate([ref[...] for ref in piece_refs], axis=0)
    return dot(mix.astype(jnp.bfloat16), rows)


def combine(me, columns, pieces, capacity, level, levels, keep, took):
    token_count, width = columns.shape[0], pieces[0].shape[1]
    owned = keep.shape[1]

    def kernel(me_ref, columns_ref, keep_ref, took_ref, *refs):
        mixed = mixing(columns_ref[...], refs[:-1], capacity).astype(jnp.bfloat16)
        refs[-1][:token_count] = mixed
        targets = [target_level(me_ref[3], me_ref[1], level, levels)]
        if levels == RELAYED:
            targets.append(me_ref[3] ^ 1)
        for index, target in enumerate(targets):
            both = keep_ref[target].astype(jnp.float32) + took_ref[target].astype(jnp.float32)
            start = token_count + index * owned
            refs[-1][start : start + owned] = both.astype(jnp.bfloat16)

    rows = token_count + (2 if levels == RELAYED else 1) * owned
    return pl.pallas_call(
        kernel,
        out_shape=jax.ShapeDtypeStruct((rows, width), jnp.bfloat16),
        in_specs=[SCALAR] + [VECTOR] * (3 + len(pieces)),
        out_specs=VECTOR,
        compiler_params=PARAMS,
        cost_estimate=pl.CostEstimate(
            flops=1_500_000_000, bytes_accessed=2_000_000, transcendentals=0
        ),
        name="combine",
    )(me, columns, keep, took, *pieces)


def merge(share, beside, across, token_count, owned):
    end = token_count + owned

    def kernel(share_ref, beside_ref, across_ref, out_ref):
        total = share_ref[:end].astype(jnp.float32) + beside_ref[:end].astype(jnp.float32)
        out_ref[:token_count] = total[:token_count].astype(jnp.bfloat16)
        last = total[token_count:] + across_ref[end:].astype(jnp.float32)
        out_ref[token_count:] = last.astype(jnp.bfloat16)

    return pl.pallas_call(
        kernel,
        out_shape=jax.ShapeDtypeStruct((end, share.shape[1]), jnp.bfloat16),
        in_specs=[VECTOR] * 3,
        out_specs=VECTOR,
        compiler_params=PARAMS,
        cost_estimate=pl.CostEstimate(
            flops=500_000_000, bytes_accessed=2_000_000, transcendentals=0
        ),
        name="merge",
    )(share, beside, across)


def finish(me, packed, pieces, capacity, expert_shares, mixer_shares, keep, took):
    token_count, width = packed.shape
    width -= LANES
    owned = keep.shape[1]
    shares = list({id(a): a for a in (*expert_shares, *(a for a, _ in mixer_shares))}.values())
    places = {id(a): index for index, a in enumerate(shares)}

    def kernel(me_ref, columns_ref, keep_ref, took_ref, *refs):
        piece_refs = refs[: len(pieces)]
        share_refs = refs[len(pieces) : -2]
        expert_ref, mixer_ref = refs[-2:]
        total = mixing(columns_ref[...], piece_refs, capacity)
        for share in expert_shares:
            total = total + share_refs[places[id(share)]][:token_count].astype(jnp.float32)
        expert_ref[...] = total.astype(jnp.bfloat16)
        level = me_ref[3]
        mixer = keep_ref[level].astype(jnp.float32) + took_ref[level].astype(jnp.float32)
        for share, slot in mixer_shares:
            start = token_count + slot * owned
            rows = share_refs[places[id(share)]][start : start + owned]
            mixer = mixer + rows.astype(jnp.float32)
        mixer_ref[...] = mixer.astype(jnp.bfloat16)

    shapes = (
        jax.ShapeDtypeStruct((token_count, width), jnp.bfloat16),
        jax.ShapeDtypeStruct(keep.shape[1:], jnp.bfloat16),
    )
    return pl.pallas_call(
        kernel,
        grid=(1,),
        out_shape=shapes,
        in_specs=[SCALAR, pl.BlockSpec((token_count, LANES), lambda i: (0, width // LANES))]
        + [whole(a) for a in (keep, took, *pieces, *shares)],
        out_specs=[whole(a) for a in shapes],
        compiler_params=PARAMS,
        cost_estimate=pl.CostEstimate(
            flops=1_500_000_000, bytes_accessed=2_000_000, transcendentals=0
        ),
        name="finish",
    )(me, packed, keep, took, *pieces, *shares)


def body(
    query_rows,
    key_rows,
    value_rows,
    query_norm_gain,
    key_gain,
    break_offset,
    mixer_out_weight,
    routed_tokens,
    expert_gain,
    routes,
    route_scores,
    gate_weight,
    up_weight,
    down_weight,
):
    expert_count = lax.axis_size("ep")
    piece_count = expert_count if expert_count <= MOST_PERMUTES else 1
    levels = lax.axis_size("tp") // CORES
    token_count = routed_tokens.shape[0]
    capacity = max(2, token_count * TOP_K // expert_count)
    slot_count = expert_count * capacity

    level_index = lax.axis_index("tp") // CORES
    outer = (level_index == 0) | (level_index == levels - 1)
    core_index = lax.axis_index("tp") % CORES
    me = jnp.stack([lax.axis_index("ep"), outer, core_index, level_index]).astype(jnp.int32)
    packed, pieces = prepare(
        me,
        routed_tokens,
        expert_gain,
        routes,
        route_scores,
        key_rows,
        value_rows,
        expert_count,
        piece_count,
        capacity,
    )
    blocks = gather_z(packed, levels)
    own = (gate_weight[0].T, up_weight[0].T, down_weight[0])
    weights = [tuple(over_core(w, step) for w in own) for step in range(1, CORES)]
    own = tuple(pltpu.with_memory_space_constraint(w, pltpu.VMEM) for w in own)
    weights = [own] + weights
    arrived = [over_ep(pieces)]
    if piece_count == 1:
        both = jnp.concatenate([key_rows, value_rows], axis=1)
        others, slots = [lax.all_gather(both, "ep", axis=0, tiled=True)], None
    else:
        others, slots = arrived[0][1:], capacity
    keep, give = attention(
        me,
        others,
        slots,
        query_rows,
        key_rows,
        value_rows,
        query_norm_gain,
        key_gain,
        break_offset,
        mixer_out_weight,
    )
    took = over_core(give, 1)

    columns = [None]
    for level in range(1, levels):
        column, picked = select(
            me, blocks[level - 1], piece_count, slot_count, capacity
        )
        columns.append(column)
        arrived.append(over_ep(picked))

    piece_rows = slot_count // piece_count

    def layer(level, **options):
        return expert_layer(arrived[level], piece_rows, weights, **options)

    def share_of(level):
        returned = over_ep(layer(level), back=True)
        return combine(me, columns[level], returned, capacity, level, levels, keep, took)

    if levels == RELAYED:
        beside = over_z(layer(1, joined=True)[0], [(0, 1), (1, 0), (2, 3), (3, 2)])
        share = share_of(2)
        inner = over_z(share, [(1, 2), (2, 1)])
        distant = over_z(share, [(0, 2), (3, 1)])
        share = share_of(3)
        nearer = over_z(share, [(0, 1), (3, 2)])
        share = merge(share, nearer, inner, token_count, keep.shape[1])
        last = over_z(share, [(1, 3), (2, 0)])
        results = layer(0, addend=beside)
        expert_shares = [inner, distant, last]
        mixer_shares = [(inner, 0), (distant, 0), (nearer, 1), (last, 0)]
    else:
        expert_shares = []
        for level in range(1, levels):
            pairs = [(partner(i, level, levels), i) for i in range(levels)]
            expert_shares.append(over_z(share_of(level), pairs))
        results = layer(0)
        mixer_shares = [(share, 0) for share in expert_shares]
    returned = over_ep(results, back=True)
    expert_output, mixer_output = finish(
        me, packed, returned, capacity, expert_shares, mixer_shares, keep, took
    )
    return (mixer_output, expert_output)


def solution(mesh):
    in_specs = (
        P("ep", "tp"),
        P("ep", "tp"),
        P("ep", "tp"),
        P(),
        P(),
        P("tp"),
        P("tp", None),
        P(("ep", "tp"), None),
        P(),
        P(("ep", "tp"), None),
        P(("ep", "tp"), None),
        P("ep", None, "tp"),
        P("ep", None, "tp"),
        P("ep", "tp", None),
    )
    out_specs = (P(("ep", "tp"), None), P(("ep", "tp"), None))
    return jax.shard_map(
        body,
        mesh=mesh,
        in_specs=in_specs,
        out_specs=out_specs,
        check_vma=False,
    )
```

```python
import jax
import jax.numpy as jnp
from jax import lax
from jax.experimental import pallas as pl
from jax.experimental.pallas import tpu as pltpu
from jax.sharding import PartitionSpec as P


HEAD_DIM = 64
TOP_K = 2
CORES = 2
LANES = 128
MOST_PERMUTES = 8


EPS = 1e-06


def partner(index, step, count):
    if count & (count - 1) == 0:
        return index ^ step
    return (index + step) % count


def relative(target, index, count):
    if count & (count - 1) == 0:
        return target ^ index
    return (target - index + count) % count


def over_ep(pieces, back=False):
    count = lax.axis_size("ep")
    if len(pieces) == 1:
        return [lax.all_to_all(pieces[0], "ep", split_axis=0, concat_axis=0, tiled=True)]
    moved = [pieces[0]]
    for step in range(1, count):
        pairs = [(i, partner(i, step, count)) for i in range(count)]
        if back:
            pairs = [(b, a) for a, b in pairs]
        moved.append(lax.ppermute(pieces[step], "ep", pairs))
    return moved


def over_z(array, pairs):
    pairs = [(a * CORES + c, b * CORES + c) for a, b in pairs for c in range(CORES)]
    return lax.ppermute(array, "tp", pairs)


RELAYED = 4
PARTS = 2


def gather_z(packed, levels):
    if levels != RELAYED:
        return [
            [over_z(packed, [(i, partner(i, step, levels)) for i in range(levels)])]
            for step in range(1, levels)
        ]
    beside = over_z(packed, [(0, 1), (1, 0), (2, 3), (3, 2)])
    across = over_z(packed, [(1, 2), (2, 1)])
    beyond = over_z(beside, [(1, 2), (2, 1)])
    second = over_z(across, [(1, 0), (2, 3)])
    third = over_z(beyond, [(1, 0), (2, 3)])
    return [[beside], [second, across], [third, beyond]]


def over_core(array, step):
    count = lax.axis_size("tp")
    pairs = [(i, i // CORES * CORES + (i + step) % CORES) for i in range(count)]
    return lax.ppermute(array, "tp", pairs)


def dot(a, b, dims=((1,), (0,)), precision=None):
    return lax.dot_general(
        a, b, (dims, ((), ())), precision=precision, preferred_element_type=jnp.float32
    )


def whole(array):
    return pl.BlockSpec(array.shape, lambda *_: (0,) * array.ndim)


VECTOR = pl.BlockSpec(memory_space=pltpu.VMEM)
REMAIN = pl.BlockSpec(memory_space=pltpu.HBM)
PARAMS = pltpu.CompilerParams(vmem_limit_bytes=16 * 1024 * 1024)


SCALAR = pl.BlockSpec(memory_space=pltpu.SMEM)


def head_norm(rows, gain):
    split = rows.astype(jnp.float32)
    mean = jnp.sum(split * split, axis=1, keepdims=True) * (1.0 / HEAD_DIM)
    return (split * lax.rsqrt(mean + EPS) * gain).astype(jnp.bfloat16)


def attention_kernel(slots, *refs):
    me_ref, offset_ref, query_ref, query_gain_ref, key_gain_ref, mixer_ref = refs[:6]
    key_ref, value_ref, *block_refs, keep_ref, give_ref, terms_ref = refs[6:]
    row_count, width = query_ref.shape
    head_count = width // HEAD_DIM
    me = me_ref[0]
    if slots is None:
        blocks = [(block_refs[0][:, :width], block_refs[0][:, width:])]
        places = [0]
    else:
        fold = block_refs[0].shape[1] // (2 * width)
        part = row_count // fold
        blocks = [(key_ref[...], value_ref[...])]
        for ref in block_refs:
            rows = ref[slots : slots + part]
            rows = jnp.concatenate(
                [rows[:, 2 * width * f : 2 * width * (f + 1)] for f in range(fold)], axis=0
            )
            blocks.append((rows[:, :width], rows[:, width:]))
        places = [partner(me, step, len(blocks)) * row_count for step in range(len(blocks))]
    query_place = me * row_count + lax.broadcasted_iota(jnp.int32, (row_count, 1), 0)
    block_rows = blocks[0][0].shape[0]
    row = lax.broadcasted_iota(jnp.int32, (block_rows, block_rows), 0)
    column = lax.broadcasted_iota(jnp.int32, (block_rows, block_rows), 1)
    later = jnp.where(row > column, 1.0, 0.0).astype(jnp.bfloat16)
    key_iota = lax.broadcasted_iota(jnp.int32, (1, block_rows), 1)
    mixed = []
    for head in range(head_count):
        cut = slice(head * HEAD_DIM, (head + 1) * HEAD_DIM)
        query = head_norm(query_ref[:, cut], query_gain_ref[...])
        rises, fails, totals, allows = [], [], [], []
        for index, (keys, _) in enumerate(blocks):
            key = head_norm(keys[:, cut], key_gain_ref[...])
            scores = dot(query, key, ((1,), (1,))) * HEAD_DIM ** (-0.5) + offset_ref[head]
            before = places[index] + key_iota < query_place
            rise = jnp.minimum(scores, 0.0) - jnp.log1p(jnp.exp(-jnp.abs(scores)))
            fail = jnp.where(before, rise - scores, 0.0)
            rises.append(rise)
            fails.append(fail)
            allows.append(before)
            totals.append(jnp.sum(fail, axis=1, keepdims=True))
        mix = jnp.zeros((row_count, HEAD_DIM), jnp.float32)
        for index, (_, values) in enumerate(blocks):
            after = jnp.zeros((row_count, 1), jnp.float32)
            for other in range(len(blocks)):
                if other != index:
                    behind = places[other] > places[index]
                    after = after + jnp.where(behind, totals[other], 0.0)
            rest = fails[index]
            for _ in range(3):
                part = rest.astype(jnp.bfloat16)
                after = after + dot(part, later)
                rest = rest - part.astype(jnp.float32)
            weights = jnp.where(allows[index], jnp.exp(rises[index] + after), 0.0)
            mix = mix + dot(weights.astype(jnp.bfloat16), values[:, cut])
        mixed.append(mix.astype(jnp.bfloat16))
    terms = dot(jnp.concatenate(mixed, axis=1), mixer_ref[...]).astype(jnp.bfloat16)
    levels, owned = keep_ref.shape[:2]
    for index in range(levels * CORES):
        terms_ref[index] = terms[index * owned : (index + 1) * owned]
    core = me_ref[2]
    for level in range(levels):
        keep_ref[level] = terms_ref[level * CORES + core]
        give_ref[level] = terms_ref[level * CORES + 1 - core]


def attention(
    me, blocks, slots, query_rows, key_rows, value_rows, query_norm_gain, key_gain, offset, mixer
):
    row_count = query_rows.shape[0]
    owners = lax.axis_size("tp")
    shape = (owners // CORES, row_count // owners, mixer.shape[1])
    args = (query_rows, query_norm_gain[None], key_gain[None], mixer, key_rows, value_rows)
    return pl.pallas_call(
        lambda *refs: attention_kernel(slots, *refs),
        out_shape=[jax.ShapeDtypeStruct(shape, jnp.bfloat16)] * 2,
        grid=(1,),
        in_specs=[SCALAR, SCALAR] + [whole(a) for a in (*args, *blocks)],
        out_specs=[VECTOR] * 2,
        scratch_shapes=[pltpu.VMEM((owners, *shape[1:]), jnp.bfloat16)],
        compiler_params=PARAMS,
        cost_estimate=pl.CostEstimate(
            flops=6_000_000_000, bytes_accessed=3_000_000, transcendentals=1_000_000
        ),
        name="attention",
    )(me, offset, *args, *blocks)


def hits(rows, slot_count, capacity):
    slots = lax.broadcasted_iota(jnp.int32, (slot_count, 1), 0).astype(jnp.float32)
    return [
        rows[TOP_K + k : TOP_K + k + 1] * capacity + rows[k : k + 1] == slots for k in range(TOP_K)
    ]


def spread(rows, tokens, out_refs, slot_count, capacity):
    piece_rows = slot_count // len(out_refs)
    picked = 0.0
    for hit in hits(rows, slot_count, capacity):
        picked = picked + jnp.where(hit, 1.0, 0.0)
    picked = picked.astype(jnp.bfloat16)
    for index, ref in enumerate(out_refs):
        part = picked[index * piece_rows : (index + 1) * piece_rows]
        ref[:piece_rows] = dot(part, tokens).astype(jnp.bfloat16)


def prepare_kernel(expert_count, capacity, me_ref, *refs):
    inputs, outputs, scratch = refs[:6], refs[6:-6], refs[-6:]
    packed_ref, *out_refs = outputs
    both_ref = scratch[4]
    tokens_ref, gain_ref, routes_ref, scores_ref = scratch[:4]
    half = both_ref.shape[1] // 2
    targets = (*scratch[:4], both_ref.at[:, :half], both_ref.at[:, half:])
    copies = [
        pltpu.make_async_copy(source, target, scratch[5].at[index])
        for index, (source, target) in enumerate(zip(inputs, targets))
    ]
    for copy in copies:
        copy.start()
    for copy in copies:
        copy.wait()
    token_count, width = tokens_ref.shape
    as_float = tokens_ref[...].astype(jnp.float32)
    mean = jnp.sum(as_float * as_float, axis=1, keepdims=True) * (1.0 / width)
    normed = (as_float * lax.rsqrt(mean + EPS) * gain_ref[...]).astype(jnp.bfloat16)
    packed_ref[:, :width] = normed
    routes = routes_ref[...]
    scores = scores_ref[...]
    experts = lax.broadcasted_iota(jnp.int32, (expert_count, 1), 0)
    row = lax.broadcasted_iota(jnp.int32, (token_count, token_count), 0)
    column = lax.broadcasted_iota(jnp.int32, (token_count, token_count), 1)
    earlier = jnp.where(row < column, 1.0, 0.0).astype(jnp.bfloat16)
    taken = jnp.zeros((expert_count, 1), jnp.float32)
    aheads, nears, weights = [], [], []
    for k in range(TOP_K):
        chosen = routes[k : k + 1]
        member = jnp.where(chosen == experts, 1.0, 0.0)
        ahead = dot(member.astype(jnp.bfloat16), earlier) + taken
        aheads.append(jnp.sum(member * ahead, axis=0, keepdims=True))
        taken = taken + jnp.sum(member, axis=1, keepdims=True)
        if len(out_refs) == 1:
            near = chosen
        else:
            near = relative(chosen, me_ref[0], expert_count)
        nears.append(near.astype(jnp.float32))
        total = 0.0
        for j in range(TOP_K):
            total = total + jnp.exp(scores[j : j + 1] - scores[k : k + 1])
        weights.append(1.0 / total)
    rows = aheads + nears + weights
    rows = jnp.concatenate(
        rows + [jnp.zeros((LANES - len(rows), token_count), jnp.float32)], axis=0
    )
    packed_ref[:, width:] = rows.T.astype(jnp.bfloat16)
    slot_count = expert_count * capacity
    spread(rows, normed, out_refs, slot_count, capacity)
    for ref in out_refs[1:]:
        fold = width // both_ref.shape[1]
        part = both_ref.shape[0] // fold
        for f in range(fold):
            columns = slice(f * both_ref.shape[1], (f + 1) * both_ref.shape[1])
            ref[capacity:, columns] = both_ref[f * part : (f + 1) * part]


def piece_shapes(count, slot_count, width):
    return [
        jax.ShapeDtypeStruct((slot_count // count, width), jnp.bfloat16) for _ in range(count)
    ]


def prepare(me, tokens, gain, routes, scores, keys, values, expert_count, piece_count, capacity):
    token_count, width = tokens.shape
    both = (keys.shape[0], keys.shape[1] + values.shape[1])
    shapes = [jax.ShapeDtypeStruct((token_count, width + LANES), jnp.bfloat16)]
    shapes += piece_shapes(piece_count, expert_count * capacity, width)
    extra = both[0] * both[1] // width
    shapes[2:] = [jax.ShapeDtypeStruct((capacity + extra, width), jnp.bfloat16)] * (piece_count - 1)
    args = (tokens, gain[None], routes.T, scores.T, keys, values)
    args = tuple(pltpu.with_memory_space_constraint(a, pltpu.HBM) for a in args)
    packed, *pieces = pl.pallas_call(
        lambda *refs: prepare_kernel(expert_count, capacity, *refs),
        out_shape=shapes,
        in_specs=[SCALAR] + [REMAIN] * len(args),
        out_specs=[VECTOR] * len(shapes),
        scratch_shapes=[pltpu.VMEM(a.shape, a.dtype) for a in args[:4]]
        + [pltpu.VMEM(both, keys.dtype), pltpu.SemaphoreType.DMA((len(args),))],
        compiler_params=PARAMS,
        cost_estimate=pl.CostEstimate(
            flops=2_000_000_000, bytes_accessed=3_000_000, transcendentals=0
        ),
        name="prepare",
    )(me, *args)
    return packed, pieces


def select(me, candidates, piece_count, slot_count, capacity):
    token_count, width = candidates[0].shape
    width -= LANES

    def kernel(me_ref, *refs):
        packed = refs[0][...]
        if len(candidates) > 1:
            packed = jnp.where(me_ref[1] == 1, packed, refs[1][...])
        columns_ref, *out_refs = refs[len(candidates) :]
        columns_ref[...] = packed[:, width:]
        rows = packed[:, width:].astype(jnp.float32).T
        spread(rows, packed[:, :width], out_refs, slot_count, capacity)

    shapes = [jax.ShapeDtypeStruct((token_count, LANES), jnp.bfloat16)]
    shapes += piece_shapes(piece_count, slot_count, width)
    columns, *pieces = pl.pallas_call(
        kernel,
        out_shape=shapes,
        in_specs=[SCALAR] + [VECTOR] * len(candidates),
        out_specs=[VECTOR] * len(shapes),
        compiler_params=PARAMS,
        cost_estimate=pl.CostEstimate(
            flops=1_500_000_000, bytes_accessed=2_000_000, transcendentals=0
        ),
        name="select",
    )(me, *candidates)
    return columns, pieces


def hold(arrays):
    def kernel(*refs):
        count = len(arrays)
        copies = [
            pltpu.make_async_copy(refs[i], refs[count + i], refs[-1].at[i]) for i in range(count)
        ]
        for copy in copies:
            copy.start()
        for copy in copies:
            copy.wait()

    return tuple(
        pl.pallas_call(
            kernel,
            out_shape=[jax.ShapeDtypeStruct(a.shape, a.dtype) for a in arrays],
            in_specs=[REMAIN] * len(arrays),
            out_specs=[VECTOR] * len(arrays),
            scratch_shapes=[pltpu.SemaphoreType.DMA((len(arrays),))],
            compiler_params=PARAMS,
            cost_estimate=pl.CostEstimate(
                flops=500_000_000, bytes_accessed=6_000_000, transcendentals=0
            ),
            name="hold",
        )(*arrays)
    )


def expert_layer(pieces, piece_rows, weights, joined=False, parts=1, terms=()):
    width = pieces[0].shape[1]
    count = len(pieces)
    row_count = count * piece_rows
    units = weights[0][0].shape[0]
    groups = len(weights)
    flat = [w for group in weights for w in group]

    def kernel(*refs):
        refs = list(refs)
        rows_refs = [refs.pop(0) for _ in pieces]
        term_refs = [refs.pop(0) for _ in terms]
        weight_refs = [refs.pop(0) for _ in flat]
        out_refs = refs
        rows = jnp.concatenate([ref[:piece_rows] for ref in rows_refs], axis=0)
        total = jnp.zeros((row_count, width), jnp.float32)
        for g in range(groups):
            gate_ref, up_ref, down_ref = weight_refs[3 * g : 3 * g + 3]
            gate = dot(rows, gate_ref[...], ((1,), (1,)))
            up = dot(rows, up_ref[...], ((1,), (1,)))
            hidden = (gate / (1.0 + jnp.exp(-gate)) * up).astype(jnp.bfloat16)
            total = total + dot(hidden, down_ref[...])
        total = total.astype(jnp.bfloat16)
        part = row_count // outputs
        wide = width // parts
        for index, ref in enumerate(out_refs):
            left = index // outputs * wide
            top = index % outputs * part
            ref[:part] = total[top : top + part, left : left + wide]
        if terms:
            me_ref, keep_ref, took_ref = term_refs
            out_refs[0][row_count:] = owed(keep_ref, took_ref, me_ref[3] ^ 1)

    outputs = 1 if joined else count
    shapes = piece_shapes(outputs, row_count, width // parts) * parts
    if terms:
        shapes = piece_shapes(1, row_count + terms[1].shape[1], width)
    results = list(
        pl.pallas_call(
            kernel,
            out_shape=shapes,
            in_specs=[VECTOR] * count
            + [SCALAR, VECTOR, VECTOR][: len(terms)]
            + [VECTOR] * len(flat),
            out_specs=[VECTOR] * len(shapes),
            compiler_params=PARAMS,
            cost_estimate=pl.CostEstimate(
                flops=6 * row_count * units * groups * width,
                bytes_accessed=6 * units * groups * width,
                transcendentals=row_count * units * groups,
            ),
            name="expert_layer",
        )(*pieces, *terms, *flat)
    )
    return [results[outputs * p : outputs * (p + 1)] for p in range(parts)]


def mixing(columns, piece_refs, capacity):
    slot_count = sum(ref.shape[0] for ref in piece_refs)
    columns = columns.astype(jnp.float32)
    slots = lax.broadcasted_iota(jnp.int32, (1, slot_count), 1).astype(jnp.float32)
    mix = 0.0
    for k in range(TOP_K):
        near = columns[:, TOP_K + k : TOP_K + k + 1]
        hit = near * capacity + columns[:, k : k + 1] == slots
        mix = mix + jnp.where(hit, columns[:, 2 * TOP_K + k : 2 * TOP_K + k + 1], 0.0)
    rows = jnp.concatenate([ref[...] for ref in piece_refs], axis=0)
    return dot(mix.astype(jnp.bfloat16), rows)


def owed(keep_ref, took_ref, target):
    both = keep_ref[target].astype(jnp.float32) + took_ref[target].astype(jnp.float32)
    return both.astype(jnp.bfloat16)


def combine(columns, pieces, capacity, level=None, part=0, terms=()):
    token_count, wide = columns.shape[0], pieces[0].shape[1]

    def kernel(columns_ref, *refs):
        piece_refs, out_ref = refs[len(terms) : -1], refs[-1]
        mixed = mixing(columns_ref[...], piece_refs, capacity).astype(jnp.bfloat16)
        out_ref[:token_count] = mixed
        if terms:
            me_ref, keep_ref, took_ref = refs[:3]
            step = 3 - me_ref[1] if level == 2 else 2 + me_ref[1]
            rows = owed(keep_ref, took_ref, me_ref[3] ^ step)
            out_ref[token_count:] = rows[:, part * wide : (part + 1) * wide]

    rows = token_count + (terms[1].shape[1] if terms else 0)
    return pl.pallas_call(
        kernel,
        out_shape=jax.ShapeDtypeStruct((rows, wide), jnp.bfloat16),
        in_specs=[VECTOR] + [SCALAR, VECTOR, VECTOR][: len(terms)] + [VECTOR] * len(pieces),
        out_specs=VECTOR,
        compiler_params=PARAMS,
        cost_estimate=pl.CostEstimate(
            flops=1_500_000_000, bytes_accessed=2_000_000, transcendentals=0
        ),
        name="combine",
    )(columns, *terms, *pieces)


def owners(me, keep, took, levels):
    def kernel(me_ref, keep_ref, took_ref, *out_refs):
        for step, ref in enumerate(out_refs):
            target = me_ref[3]
            if step > 0:
                if levels & (levels - 1) == 0:
                    target = target ^ step
                else:
                    target = (target - step + levels) % levels
            both = keep_ref[target].astype(jnp.float32) + took_ref[target].astype(jnp.float32)
            ref[...] = both.astype(ref.dtype)

    shapes = [
        jax.ShapeDtypeStruct(keep.shape[1:], jnp.bfloat16 if step else jnp.float32)
        for step in range(levels)
    ]
    return pl.pallas_call(
        kernel,
        out_shape=shapes,
        in_specs=[SCALAR] + [VECTOR] * 2,
        out_specs=[VECTOR] * levels,
        compiler_params=PARAMS,
        cost_estimate=pl.CostEstimate(
            flops=500_000_000, bytes_accessed=1_000_000, transcendentals=0
        ),
        name="owners",
    )(me, keep, took)


def merge(share, beside, count=1):
    rows = share.shape[0]

    def kernel(share_ref, beside_ref, *out_refs):
        total = share_ref[...].astype(jnp.float32) + beside_ref[:rows].astype(jnp.float32)
        total = total.astype(jnp.bfloat16)
        part = rows // count
        for index, ref in enumerate(out_refs):
            ref[...] = total[index * part : (index + 1) * part]

    shapes = piece_shapes(count, *share.shape)
    return pl.pallas_call(
        kernel,
        out_shape=shapes,
        in_specs=[VECTOR] * 2,
        out_specs=[VECTOR] * count,
        compiler_params=PARAMS,
        cost_estimate=pl.CostEstimate(
            flops=500_000_000, bytes_accessed=1_000_000, transcendentals=0
        ),
        name="merge",
    )(share, beside)


def finish(me, packed, pieces, capacity, shares, keep, took, mixers):
    token_count, width = packed.shape
    width -= LANES
    owned = keep.shape[1]

    def kernel(me_ref, columns_ref, keep_ref, took_ref, *refs):
        piece_refs = refs[: len(pieces)]
        share_refs = refs[len(pieces) : len(pieces) + len(shares)]
        mixer_refs = refs[len(pieces) + len(shares) : -2]
        expert_ref, mixer_ref = refs[-2:]
        total = mixing(columns_ref[...], piece_refs, capacity)
        level = me_ref[3]
        mixer = keep_ref[level].astype(jnp.float32) + took_ref[level].astype(jnp.float32)
        for ref in mixer_refs:
            mixer = mixer + ref[...].astype(jnp.float32)
        wide = share_refs[0].shape[1]
        for left in range(0, width, wide):
            part = total[:, left : left + wide]
            terms = mixer[:, left : left + wide]
            for ref, (place, _) in zip(share_refs, shares):
                if place * wide == left:
                    part = part + ref[:token_count].astype(jnp.float32)
                    if ref.shape[0] > token_count:
                        terms = terms + ref[token_count:].astype(jnp.float32)
            expert_ref[:, left : left + wide] = part.astype(jnp.bfloat16)
            mixer_ref[:, left : left + wide] = terms.astype(jnp.bfloat16)

    shapes = (
        jax.ShapeDtypeStruct((token_count, width), jnp.bfloat16),
        jax.ShapeDtypeStruct(keep.shape[1:], jnp.bfloat16),
    )
    arrays = (keep, took, *pieces, *(share for _, share in shares))
    ends = [
        pl.BlockSpec((owned, width), lambda i, a=a: (a.shape[0] // owned - 1, 0)) for a in mixers
    ]
    return pl.pallas_call(
        kernel,
        grid=(1,),
        out_shape=shapes,
        in_specs=[SCALAR, pl.BlockSpec((token_count, LANES), lambda i: (0, width // LANES))]
        + [whole(a) for a in arrays[: -len(shares)]]
        + [VECTOR] * len(shares)
        + ends,
        out_specs=[whole(a) for a in shapes],
        compiler_params=PARAMS,
        cost_estimate=pl.CostEstimate(
            flops=1_500_000_000, bytes_accessed=2_000_000, transcendentals=0
        ),
        name="finish",
    )(me, packed, *arrays, *mixers)


def body(
    query_rows,
    key_rows,
    value_rows,
    query_norm_gain,
    key_gain,
    break_offset,
    mixer_out_weight,
    routed_tokens,
    expert_gain,
    routes,
    route_scores,
    gate_weight,
    up_weight,
    down_weight,
):
    expert_count = lax.axis_size("ep")
    piece_count = expert_count if expert_count <= MOST_PERMUTES else 1
    levels = lax.axis_size("tp") // CORES
    token_count = routed_tokens.shape[0]
    capacity = max(2, token_count * TOP_K // expert_count)
    slot_count = expert_count * capacity

    level_index = lax.axis_index("tp") // CORES
    outer = (level_index == 0) | (level_index == levels - 1)
    core_index = lax.axis_index("tp") % CORES
    me = jnp.stack([lax.axis_index("ep"), outer, core_index, level_index]).astype(jnp.int32)
    packed, pieces = prepare(
        me,
        routed_tokens,
        expert_gain,
        routes,
        route_scores,
        key_rows,
        value_rows,
        expert_count,
        piece_count,
        capacity,
    )
    blocks = gather_z(packed, levels)
    own = (gate_weight[0].T, up_weight[0].T, down_weight[0])
    weights = [tuple(over_core(w, step) for w in own) for step in range(1, CORES)]
    own = tuple(pltpu.with_memory_space_constraint(w, pltpu.VMEM) for w in own)
    weights = [own] + [hold(group) for group in weights]
    arrived = [over_ep(pieces)]
    if piece_count == 1:
        both = jnp.concatenate([key_rows, value_rows], axis=1)
        others, slots = [lax.all_gather(both, "ep", axis=0, tiled=True)], None
    else:
        others, slots = arrived[0][1:], capacity
    keep, give = attention(
        me,
        others,
        slots,
        query_rows,
        key_rows,
        value_rows,
        query_norm_gain,
        key_gain,
        break_offset,
        mixer_out_weight,
    )
    took = over_core(give, 1)

    columns = [None]
    for level in range(1, levels):
        column, picked = select(
            me, blocks[level - 1], piece_count, slot_count, capacity
        )
        columns.append(column)
        arrived.append(over_ep(picked))

    piece_rows = slot_count // piece_count
    terms = (me, keep, took)

    def layer(level, **options):
        return expert_layer(arrived[level], piece_rows, weights, **options)

    def shares_of(level, parts, **options):
        shares = []
        for part, results in enumerate(layer(level, parts=parts)):
            returned = over_ep(results, back=True)
            shares.append(
                combine(columns[level], returned, capacity, level, part, **options)
            )
        return shares

    shares = []
    if levels == RELAYED:
        results = layer(1, joined=True, terms=terms)[0][0]
        beside = over_z(results, [(0, 1), (1, 0), (2, 3), (3, 2)])
        mixers = [beside]
        for level, pairs in ((2, [(1, 2), (2, 1)]), (3, [(1, 3), (2, 0)])):
            for part, share in enumerate(shares_of(level, PARTS, terms=terms)):
                nearer = over_z(share, [(0, 1), (3, 2)])
                (share,) = merge(share, nearer)
                shares.append((part, over_z(share, pairs)))
        results = layer(0, joined=True)[0][0]
        results = merge(results, beside, piece_count)
    else:
        mixers = []
        far_terms = owners(me, keep, took, levels)
        for level in range(1, levels):
            pairs = [(partner(i, level, levels), i) for i in range(levels)]
            shares.append((0, over_z(shares_of(level, 1)[0], pairs)))
            mixers.append(over_z(far_terms[level], pairs))
        results = layer(0)[0]
    returned = over_ep(results, back=True)
    expert_output, mixer_output = finish(
        me, packed, returned, capacity, shares, keep, took, mixers
    )
    return (mixer_output, expert_output)


def solution(mesh):
    in_specs = (
        P("ep", "tp"),
        P("ep", "tp"),
        P("ep", "tp"),
        P(),
        P(),
        P("tp"),
        P("tp", None),
        P(("ep", "tp"), None),
        P(),
        P(("ep", "tp"), None),
        P(("ep", "tp"), None),
        P("ep", None, "tp"),
        P("ep", None, "tp"),
        P("ep", "tp", None),
    )
    out_specs = (P(("ep", "tp"), None), P(("ep", "tp"), None))
    return jax.shard_map(
        body,
        mesh=mesh,
        in_specs=in_specs,
        out_specs=out_specs,
        check_vma=False,
    )
```

```python
import jax
import jax.numpy as jnp
from jax import lax
from jax.experimental import pallas as pl
from jax.experimental.pallas import tpu as pltpu
from jax.sharding import PartitionSpec as P


HEAD_DIM = 64
TOP_K = 2
CORES = 2
LANES = 128
MOST_PERMUTES = 8


EPS = 1e-06


def partner(index, step, count):
    if count & (count - 1) == 0:
        return index ^ step
    return (index + step) % count


def relative(target, index, count):
    if count & (count - 1) == 0:
        return target ^ index
    return (target - index + count) % count


def over_ep(pieces, back=False):
    count = lax.axis_size("ep")
    if len(pieces) == 1:
        return [lax.all_to_all(pieces[0], "ep", split_axis=0, concat_axis=0, tiled=True)]
    moved = [pieces[0]]
    for step in range(1, count):
        pairs = [(i, partner(i, step, count)) for i in range(count)]
        if back:
            pairs = [(b, a) for a, b in pairs]
        moved.append(lax.ppermute(pieces[step], "ep", pairs))
    return moved


def over_z(array, pairs):
    pairs = [(a * CORES + c, b * CORES + c) for a, b in pairs for c in range(CORES)]
    return lax.ppermute(array, "tp", pairs)


RELAYED = 4
PARTS = 2


def gather_z(packed, levels):
    if levels != RELAYED:
        return [
            [over_z(packed, [(i, partner(i, step, levels)) for i in range(levels)])]
            for step in range(1, levels)
        ]
    beside = over_z(packed, [(0, 1), (1, 0), (2, 3), (3, 2)])
    across = over_z(packed, [(1, 2), (2, 1)])
    beyond = over_z(beside, [(1, 2), (2, 1)])
    second = over_z(across, [(1, 0), (2, 3)])
    third = over_z(beyond, [(1, 0), (2, 3)])
    return [[beside], [second, across], [third, beyond]]


def over_core(array, step):
    count = lax.axis_size("tp")
    pairs = [(i, i // CORES * CORES + (i + step) % CORES) for i in range(count)]
    return lax.ppermute(array, "tp", pairs)


def dot(a, b, dims=((1,), (0,)), precision=None):
    return lax.dot_general(
        a, b, (dims, ((), ())), precision=precision, preferred_element_type=jnp.float32
    )


def whole(array):
    return pl.BlockSpec(array.shape, lambda *_: (0,) * array.ndim)


VECTOR = pl.BlockSpec(memory_space=pltpu.VMEM)
REMAIN = pl.BlockSpec(memory_space=pltpu.HBM)
PARAMS = pltpu.CompilerParams(vmem_limit_bytes=16 * 1024 * 1024)


SCALAR = pl.BlockSpec(memory_space=pltpu.SMEM)


def head_norm(rows, gain):
    split = rows.astype(jnp.float32)
    mean = jnp.sum(split * split, axis=1, keepdims=True) * (1.0 / HEAD_DIM)
    return (split * lax.rsqrt(mean + EPS) * gain).astype(jnp.bfloat16)


def attention_kernel(slots, *refs):
    me_ref, offset_ref, query_ref, query_gain_ref, key_gain_ref, mixer_ref = refs[:6]
    key_ref, value_ref, *block_refs, keep_ref, give_ref, terms_ref = refs[6:]
    row_count, width = query_ref.shape
    head_count = width // HEAD_DIM
    me = me_ref[0]
    if slots is None:
        blocks = [(block_refs[0][:, :width], block_refs[0][:, width:])]
        places = [0]
    else:
        fold = block_refs[0].shape[1] // (2 * width)
        part = row_count // fold
        blocks = [(key_ref[...], value_ref[...])]
        for ref in block_refs:
            rows = ref[slots : slots + part]
            rows = jnp.concatenate(
                [rows[:, 2 * width * f : 2 * width * (f + 1)] for f in range(fold)], axis=0
            )
            blocks.append((rows[:, :width], rows[:, width:]))
        places = [partner(me, step, len(blocks)) * row_count for step in range(len(blocks))]
    query_place = me * row_count + lax.broadcasted_iota(jnp.int32, (row_count, 1), 0)
    block_rows = blocks[0][0].shape[0]
    row = lax.broadcasted_iota(jnp.int32, (block_rows, block_rows), 0)
    column = lax.broadcasted_iota(jnp.int32, (block_rows, block_rows), 1)
    later = jnp.where(row > column, 1.0, 0.0).astype(jnp.bfloat16)
    key_iota = lax.broadcasted_iota(jnp.int32, (1, block_rows), 1)
    mixed = []
    for head in range(head_count):
        cut = slice(head * HEAD_DIM, (head + 1) * HEAD_DIM)
        query = head_norm(query_ref[:, cut], query_gain_ref[...])
        rises, fails, totals, allows = [], [], [], []
        for index, (keys, _) in enumerate(blocks):
            key = head_norm(keys[:, cut], key_gain_ref[...])
            scores = dot(query, key, ((1,), (1,))) * HEAD_DIM ** (-0.5) + offset_ref[head]
            before = places[index] + key_iota < query_place
            rise = jnp.minimum(scores, 0.0) - jnp.log1p(jnp.exp(-jnp.abs(scores)))
            fail = jnp.where(before, rise - scores, 0.0)
            rises.append(rise)
            fails.append(fail)
            allows.append(before)
            totals.append(jnp.sum(fail, axis=1, keepdims=True))
        mix = jnp.zeros((row_count, HEAD_DIM), jnp.float32)
        for index, (_, values) in enumerate(blocks):
            after = jnp.zeros((row_count, 1), jnp.float32)
            for other in range(len(blocks)):
                if other != index:
                    behind = places[other] > places[index]
                    after = after + jnp.where(behind, totals[other], 0.0)
            rest = fails[index]
            for _ in range(3):
                part = rest.astype(jnp.bfloat16)
                after = after + dot(part, later)
                rest = rest - part.astype(jnp.float32)
            weights = jnp.where(allows[index], jnp.exp(rises[index] + after), 0.0)
            mix = mix + dot(weights.astype(jnp.bfloat16), values[:, cut])
        mixed.append(mix.astype(jnp.bfloat16))
    terms = dot(jnp.concatenate(mixed, axis=1), mixer_ref[...]).astype(jnp.bfloat16)
    levels, owned = keep_ref.shape[:2]
    for index in range(levels * CORES):
        terms_ref[index] = terms[index * owned : (index + 1) * owned]
    core = me_ref[2]
    for level in range(levels):
        keep_ref[level] = terms_ref[level * CORES + core]
        give_ref[level] = terms_ref[level * CORES + 1 - core]


def attention(
    me, blocks, slots, query_rows, key_rows, value_rows, query_norm_gain, key_gain, offset, mixer
):
    row_count = query_rows.shape[0]
    owners = lax.axis_size("tp")
    shape = (owners // CORES, row_count // owners, mixer.shape[1])
    args = (query_rows, query_norm_gain[None], key_gain[None], mixer, key_rows, value_rows)
    return pl.pallas_call(
        lambda *refs: attention_kernel(slots, *refs),
        out_shape=[jax.ShapeDtypeStruct(shape, jnp.bfloat16)] * 2,
        grid=(1,),
        in_specs=[SCALAR, SCALAR] + [whole(a) for a in (*args, *blocks)],
        out_specs=[VECTOR] * 2,
        scratch_shapes=[pltpu.VMEM((owners, *shape[1:]), jnp.bfloat16)],
        compiler_params=PARAMS,
        cost_estimate=pl.CostEstimate(
            flops=6_000_000_000, bytes_accessed=3_000_000, transcendentals=1_000_000
        ),
        name="attention",
    )(me, offset, *args, *blocks)


def hits(rows, slot_count, capacity):
    slots = lax.broadcasted_iota(jnp.int32, (slot_count, 1), 0).astype(jnp.float32)
    return [
        rows[TOP_K + k : TOP_K + k + 1] * capacity + rows[k : k + 1] == slots for k in range(TOP_K)
    ]


def spread(rows, tokens, out_refs, slot_count, capacity):
    piece_rows = slot_count // len(out_refs)
    picked = 0.0
    for hit in hits(rows, slot_count, capacity):
        picked = picked + jnp.where(hit, 1.0, 0.0)
    picked = picked.astype(jnp.bfloat16)
    for index, ref in enumerate(out_refs):
        part = picked[index * piece_rows : (index + 1) * piece_rows]
        ref[:piece_rows] = dot(part, tokens).astype(jnp.bfloat16)


def prepare_kernel(expert_count, capacity, me_ref, *refs):
    inputs, outputs, scratch = refs[:6], refs[6:-6], refs[-6:]
    packed_ref, mix_ref, *out_refs = outputs
    both_ref = scratch[4]
    tokens_ref, gain_ref, routes_ref, scores_ref = scratch[:4]
    half = both_ref.shape[1] // 2
    targets = (*scratch[:4], both_ref.at[:, :half], both_ref.at[:, half:])
    copies = [
        pltpu.make_async_copy(source, target, scratch[5].at[index])
        for index, (source, target) in enumerate(zip(inputs, targets))
    ]
    for copy in copies:
        copy.start()
    for copy in copies:
        copy.wait()
    token_count, width = tokens_ref.shape
    as_float = tokens_ref[...].astype(jnp.float32)
    mean = jnp.sum(as_float * as_float, axis=1, keepdims=True) * (1.0 / width)
    normed = (as_float * lax.rsqrt(mean + EPS) * gain_ref[...]).astype(jnp.bfloat16)
    packed_ref[:, :width] = normed
    routes = routes_ref[...]
    scores = scores_ref[...]
    experts = lax.broadcasted_iota(jnp.int32, (expert_count, 1), 0)
    row = lax.broadcasted_iota(jnp.int32, (token_count, token_count), 0)
    column = lax.broadcasted_iota(jnp.int32, (token_count, token_count), 1)
    earlier = jnp.where(row < column, 1.0, 0.0).astype(jnp.bfloat16)
    taken = jnp.zeros((expert_count, 1), jnp.float32)
    aheads, nears, weights = [], [], []
    for k in range(TOP_K):
        chosen = routes[k : k + 1]
        member = jnp.where(chosen == experts, 1.0, 0.0)
        ahead = dot(member.astype(jnp.bfloat16), earlier) + taken
        aheads.append(jnp.sum(member * ahead, axis=0, keepdims=True))
        taken = taken + jnp.sum(member, axis=1, keepdims=True)
        if len(out_refs) == 1:
            near = chosen
        else:
            near = relative(chosen, me_ref[0], expert_count)
        nears.append(near.astype(jnp.float32))
        total = 0.0
        for j in range(TOP_K):
            total = total + jnp.exp(scores[j : j + 1] - scores[k : k + 1])
        weights.append(1.0 / total)
    rows = aheads + nears + weights
    rows = jnp.concatenate(
        rows + [jnp.zeros((LANES - len(rows), token_count), jnp.float32)], axis=0
    )
    columns = rows.T.astype(jnp.bfloat16)
    packed_ref[:, width:] = columns
    slot_count = expert_count * capacity
    mix_ref[...] = weigh(columns, slot_count, capacity)
    spread(rows, normed, out_refs, slot_count, capacity)
    for ref in out_refs[1:]:
        fold = width // both_ref.shape[1]
        part = both_ref.shape[0] // fold
        for f in range(fold):
            columns = slice(f * both_ref.shape[1], (f + 1) * both_ref.shape[1])
            ref[capacity:, columns] = both_ref[f * part : (f + 1) * part]


def piece_shapes(count, slot_count, width):
    return [
        jax.ShapeDtypeStruct((slot_count // count, width), jnp.bfloat16) for _ in range(count)
    ]


def prepare(me, tokens, gain, routes, scores, keys, values, expert_count, piece_count, capacity):
    token_count, width = tokens.shape
    both = (keys.shape[0], keys.shape[1] + values.shape[1])
    shapes = [jax.ShapeDtypeStruct((token_count, width + LANES), jnp.bfloat16)]
    shapes += [jax.ShapeDtypeStruct((token_count, expert_count * capacity), jnp.bfloat16)]
    shapes += piece_shapes(piece_count, expert_count * capacity, width)
    extra = both[0] * both[1] // width
    shapes[3:] = [jax.ShapeDtypeStruct((capacity + extra, width), jnp.bfloat16)] * (piece_count - 1)
    args = (tokens, gain[None], routes.T, scores.T, keys, values)
    args = tuple(pltpu.with_memory_space_constraint(a, pltpu.HBM) for a in args)
    packed, mix, *pieces = pl.pallas_call(
        lambda *refs: prepare_kernel(expert_count, capacity, *refs),
        out_shape=shapes,
        in_specs=[SCALAR] + [REMAIN] * len(args),
        out_specs=[VECTOR] * len(shapes),
        scratch_shapes=[pltpu.VMEM(a.shape, a.dtype) for a in args[:4]]
        + [pltpu.VMEM(both, keys.dtype), pltpu.SemaphoreType.DMA((len(args),))],
        compiler_params=PARAMS,
        cost_estimate=pl.CostEstimate(
            flops=2_000_000_000, bytes_accessed=3_000_000, transcendentals=0
        ),
        name="prepare",
    )(me, *args)
    return packed, mix, pieces


def select(me, candidates, piece_count, slot_count, capacity):
    token_count, width = candidates[0].shape
    width -= LANES

    def kernel(me_ref, *refs):
        packed = refs[0][...]
        if len(candidates) > 1:
            packed = jnp.where(me_ref[1] == 1, packed, refs[1][...])
        mix_ref, *out_refs = refs[len(candidates) :]
        mix_ref[...] = weigh(packed[:, width:], slot_count, capacity)
        rows = packed[:, width:].astype(jnp.float32).T
        spread(rows, packed[:, :width], out_refs, slot_count, capacity)

    shapes = [jax.ShapeDtypeStruct((token_count, slot_count), jnp.bfloat16)]
    shapes += piece_shapes(piece_count, slot_count, width)
    mix, *pieces = pl.pallas_call(
        kernel,
        out_shape=shapes,
        in_specs=[SCALAR] + [VECTOR] * len(candidates),
        out_specs=[VECTOR] * len(shapes),
        compiler_params=PARAMS,
        cost_estimate=pl.CostEstimate(
            flops=1_500_000_000, bytes_accessed=2_000_000, transcendentals=0
        ),
        name="select",
    )(me, *candidates)
    return mix, pieces


def hold(arrays):
    def kernel(*refs):
        count = len(arrays)
        copies = [
            pltpu.make_async_copy(refs[i], refs[count + i], refs[-1].at[i]) for i in range(count)
        ]
        for copy in copies:
            copy.start()
        for copy in copies:
            copy.wait()

    return tuple(
        pl.pallas_call(
            kernel,
            out_shape=[jax.ShapeDtypeStruct(a.shape, a.dtype) for a in arrays],
            in_specs=[REMAIN] * len(arrays),
            out_specs=[VECTOR] * len(arrays),
            scratch_shapes=[pltpu.SemaphoreType.DMA((len(arrays),))],
            compiler_params=PARAMS,
            cost_estimate=pl.CostEstimate(
                flops=500_000_000, bytes_accessed=6_000_000, transcendentals=0
            ),
            name="hold",
        )(*arrays)
    )


def expert_layer(pieces, piece_rows, weights, joined=False, parts=1, terms=()):
    width = pieces[0].shape[1]
    count = len(pieces)
    row_count = count * piece_rows
    units = weights[0][0].shape[0]
    groups = len(weights)
    flat = [w for group in weights for w in group]

    def kernel(*refs):
        refs = list(refs)
        rows_refs = [refs.pop(0) for _ in pieces]
        term_refs = [refs.pop(0) for _ in terms]
        weight_refs = [refs.pop(0) for _ in flat]
        out_refs = refs
        rows = jnp.concatenate([ref[:piece_rows] for ref in rows_refs], axis=0)
        total = jnp.zeros((row_count, width), jnp.float32)
        for g in range(groups):
            gate_ref, up_ref, down_ref = weight_refs[3 * g : 3 * g + 3]
            gate = dot(rows, gate_ref[...], ((1,), (1,)))
            up = dot(rows, up_ref[...], ((1,), (1,)))
            hidden = (gate / (1.0 + jnp.exp(-gate)) * up).astype(jnp.bfloat16)
            total = total + dot(hidden, down_ref[...])
        total = total.astype(jnp.bfloat16)
        part = row_count // outputs
        wide = width // parts
        for index, ref in enumerate(out_refs):
            left = index // outputs * wide
            top = index % outputs * part
            ref[:part] = total[top : top + part, left : left + wide]
        if terms:
            me_ref, keep_ref, took_ref = term_refs
            out_refs[0][row_count:] = owed(keep_ref, took_ref, me_ref[3] ^ 1)

    outputs = 1 if joined else count
    shapes = piece_shapes(outputs, row_count, width // parts) * parts
    if terms:
        shapes = piece_shapes(1, row_count + terms[1].shape[1], width)
    results = list(
        pl.pallas_call(
            kernel,
            out_shape=shapes,
            in_specs=[VECTOR] * count
            + [SCALAR, VECTOR, VECTOR][: len(terms)]
            + [VECTOR] * len(flat),
            out_specs=[VECTOR] * len(shapes),
            compiler_params=PARAMS,
            cost_estimate=pl.CostEstimate(
                flops=6 * row_count * units * groups * width,
                bytes_accessed=6 * units * groups * width,
                transcendentals=row_count * units * groups,
            ),
            name="expert_layer",
        )(*pieces, *terms, *flat)
    )
    return [results[outputs * p : outputs * (p + 1)] for p in range(parts)]


def weigh(columns, slot_count, capacity):
    columns = columns.astype(jnp.float32)
    slots = lax.broadcasted_iota(jnp.int32, (1, slot_count), 1).astype(jnp.float32)
    mix = 0.0
    for k in range(TOP_K):
        near = columns[:, TOP_K + k : TOP_K + k + 1]
        hit = near * capacity + columns[:, k : k + 1] == slots
        mix = mix + jnp.where(hit, columns[:, 2 * TOP_K + k : 2 * TOP_K + k + 1], 0.0)
    return mix.astype(jnp.bfloat16)


def mixing(mix, piece_refs):
    return dot(mix, jnp.concatenate([ref[...] for ref in piece_refs], axis=0))


def owed(keep_ref, took_ref, target):
    both = keep_ref[target].astype(jnp.float32) + took_ref[target].astype(jnp.float32)
    return both.astype(jnp.bfloat16)


def combine(mix, pieces, level=None, part=0, terms=()):
    token_count, wide = mix.shape[0], pieces[0].shape[1]

    def kernel(mix_ref, *refs):
        piece_refs, out_ref = refs[len(terms) : -1], refs[-1]
        mixed = mixing(mix_ref[...], piece_refs).astype(jnp.bfloat16)
        out_ref[:token_count] = mixed
        if terms:
            me_ref, keep_ref, took_ref = refs[:3]
            step = 3 - me_ref[1] if level == 2 else 2 + me_ref[1]
            rows = owed(keep_ref, took_ref, me_ref[3] ^ step)
            out_ref[token_count:] = rows[:, part * wide : (part + 1) * wide]

    rows = token_count + (terms[1].shape[1] if terms else 0)
    return pl.pallas_call(
        kernel,
        out_shape=jax.ShapeDtypeStruct((rows, wide), jnp.bfloat16),
        in_specs=[VECTOR] + [SCALAR, VECTOR, VECTOR][: len(terms)] + [VECTOR] * len(pieces),
        out_specs=VECTOR,
        compiler_params=PARAMS,
        cost_estimate=pl.CostEstimate(
            flops=1_500_000_000, bytes_accessed=2_000_000, transcendentals=0
        ),
        name="combine",
    )(mix, *terms, *pieces)


def owners(me, keep, took, levels):
    def kernel(me_ref, keep_ref, took_ref, *out_refs):
        for step, ref in enumerate(out_refs):
            target = me_ref[3]
            if step > 0:
                if levels & (levels - 1) == 0:
                    target = target ^ step
                else:
                    target = (target - step + levels) % levels
            both = keep_ref[target].astype(jnp.float32) + took_ref[target].astype(jnp.float32)
            ref[...] = both.astype(ref.dtype)

    shapes = [
        jax.ShapeDtypeStruct(keep.shape[1:], jnp.bfloat16 if step else jnp.float32)
        for step in range(levels)
    ]
    return pl.pallas_call(
        kernel,
        out_shape=shapes,
        in_specs=[SCALAR] + [VECTOR] * 2,
        out_specs=[VECTOR] * levels,
        compiler_params=PARAMS,
        cost_estimate=pl.CostEstimate(
            flops=500_000_000, bytes_accessed=1_000_000, transcendentals=0
        ),
        name="owners",
    )(me, keep, took)


def merge(share, beside, count=1):
    rows = share.shape[0]

    def kernel(share_ref, beside_ref, *out_refs):
        total = share_ref[...].astype(jnp.float32) + beside_ref[:rows].astype(jnp.float32)
        total = total.astype(jnp.bfloat16)
        part = rows // count
        for index, ref in enumerate(out_refs):
            ref[...] = total[index * part : (index + 1) * part]

    shapes = piece_shapes(count, *share.shape)
    return pl.pallas_call(
        kernel,
        out_shape=shapes,
        in_specs=[VECTOR] * 2,
        out_specs=[VECTOR] * count,
        compiler_params=PARAMS,
        cost_estimate=pl.CostEstimate(
            flops=500_000_000, bytes_accessed=1_000_000, transcendentals=0
        ),
        name="merge",
    )(share, beside)


def finish(me, mix, pieces, shares, keep, took, mixers):
    token_count = mix.shape[0]
    width = keep.shape[2]
    owned = keep.shape[1]

    def kernel(me_ref, mix_ref, keep_ref, took_ref, *refs):
        piece_refs = refs[: len(pieces)]
        share_refs = refs[len(pieces) : len(pieces) + len(shares)]
        mixer_refs = refs[len(pieces) + len(shares) : -2]
        expert_ref, mixer_ref = refs[-2:]
        total = mixing(mix_ref[...], piece_refs)
        level = me_ref[3]
        mixer = keep_ref[level].astype(jnp.float32) + took_ref[level].astype(jnp.float32)
        for ref in mixer_refs:
            mixer = mixer + ref[...].astype(jnp.float32)
        wide = share_refs[0].shape[1]
        for left in range(0, width, wide):
            part = total[:, left : left + wide]
            terms = mixer[:, left : left + wide]
            for ref, (place, _) in zip(share_refs, shares):
                if place * wide == left:
                    part = part + ref[:token_count].astype(jnp.float32)
                    if ref.shape[0] > token_count:
                        terms = terms + ref[token_count:].astype(jnp.float32)
            expert_ref[:, left : left + wide] = part.astype(jnp.bfloat16)
            mixer_ref[:, left : left + wide] = terms.astype(jnp.bfloat16)

    shapes = (
        jax.ShapeDtypeStruct((token_count, width), jnp.bfloat16),
        jax.ShapeDtypeStruct(keep.shape[1:], jnp.bfloat16),
    )
    arrays = (keep, took, *pieces, *(share for _, share in shares))
    ends = [
        pl.BlockSpec((owned, width), lambda i, a=a: (a.shape[0] // owned - 1, 0)) for a in mixers
    ]
    return pl.pallas_call(
        kernel,
        grid=(1,),
        out_shape=shapes,
        in_specs=[SCALAR]
        + [whole(a) for a in (mix, keep, took)]
        + [VECTOR] * (len(pieces) + len(shares))
        + ends,
        out_specs=[whole(a) for a in shapes],
        compiler_params=PARAMS,
        cost_estimate=pl.CostEstimate(
            flops=1_500_000_000, bytes_accessed=2_000_000, transcendentals=0
        ),
        name="finish",
    )(me, mix, *arrays, *mixers)


def body(
    query_rows,
    key_rows,
    value_rows,
    query_norm_gain,
    key_gain,
    break_offset,
    mixer_out_weight,
    routed_tokens,
    expert_gain,
    routes,
    route_scores,
    gate_weight,
    up_weight,
    down_weight,
):
    expert_count = lax.axis_size("ep")
    piece_count = expert_count if expert_count <= MOST_PERMUTES else 1
    levels = lax.axis_size("tp") // CORES
    token_count = routed_tokens.shape[0]
    capacity = max(2, token_count * TOP_K // expert_count)
    slot_count = expert_count * capacity

    level_index = lax.axis_index("tp") // CORES
    outer = (level_index == 0) | (level_index == levels - 1)
    core_index = lax.axis_index("tp") % CORES
    me = jnp.stack([lax.axis_index("ep"), outer, core_index, level_index]).astype(jnp.int32)
    packed, mix, pieces = prepare(
        me,
        routed_tokens,
        expert_gain,
        routes,
        route_scores,
        key_rows,
        value_rows,
        expert_count,
        piece_count,
        capacity,
    )
    blocks = gather_z(packed, levels)
    own = (gate_weight[0].T, up_weight[0].T, down_weight[0])
    weights = [tuple(over_core(w, step) for w in own) for step in range(1, CORES)]
    own = tuple(pltpu.with_memory_space_constraint(w, pltpu.VMEM) for w in own)
    weights = [own] + [hold(group) for group in weights]
    arrived = [over_ep(pieces)]
    if piece_count == 1:
        both = jnp.concatenate([key_rows, value_rows], axis=1)
        others, slots = [lax.all_gather(both, "ep", axis=0, tiled=True)], None
    else:
        others, slots = arrived[0][1:], capacity
    keep, give = attention(
        me,
        others,
        slots,
        query_rows,
        key_rows,
        value_rows,
        query_norm_gain,
        key_gain,
        break_offset,
        mixer_out_weight,
    )
    took = over_core(give, 1)

    mixes = [mix]
    for level in range(1, levels):
        mix, picked = select(
            me, blocks[level - 1], piece_count, slot_count, capacity
        )
        mixes.append(mix)
        arrived.append(over_ep(picked))

    piece_rows = slot_count // piece_count
    terms = (me, keep, took)

    def layer(level, **options):
        return expert_layer(arrived[level], piece_rows, weights, **options)

    def shares_of(level, parts, **options):
        shares = []
        for part, results in enumerate(layer(level, parts=parts)):
            returned = over_ep(results, back=True)
            shares.append(
                combine(mixes[level], returned, level, part, **options)
            )
        return shares

    shares = []
    if levels == RELAYED:
        results = layer(1, joined=True, terms=terms)[0][0]
        beside = over_z(results, [(0, 1), (1, 0), (2, 3), (3, 2)])
        mixers = [beside]
        for level, pairs in ((2, [(1, 2), (2, 1)]), (3, [(1, 3), (2, 0)])):
            for part, share in enumerate(shares_of(level, PARTS, terms=terms)):
                nearer = over_z(share, [(0, 1), (3, 2)])
                (share,) = merge(share, nearer)
                shares.append((part, over_z(share, pairs)))
        results = layer(0, joined=True)[0][0]
        results = merge(results, beside, piece_count)
    else:
        mixers = []
        far_terms = owners(me, keep, took, levels)
        for level in range(1, levels):
            pairs = [(partner(i, level, levels), i) for i in range(levels)]
            shares.append((0, over_z(shares_of(level, 1)[0], pairs)))
            mixers.append(over_z(far_terms[level], pairs))
        results = layer(0)[0]
    returned = over_ep(results, back=True)
    expert_output, mixer_output = finish(
        me, mixes[0], returned, shares, keep, took, mixers
    )
    return (mixer_output, expert_output)


def solution(mesh):
    in_specs = (
        P("ep", "tp"),
        P("ep", "tp"),
        P("ep", "tp"),
        P(),
        P(),
        P("tp"),
        P("tp", None),
        P(("ep", "tp"), None),
        P(),
        P(("ep", "tp"), None),
        P(("ep", "tp"), None),
        P("ep", None, "tp"),
        P("ep", None, "tp"),
        P("ep", "tp", None),
    )
    out_specs = (P(("ep", "tp"), None), P(("ep", "tp"), None))
    return jax.shard_map(
        body,
        mesh=mesh,
        in_specs=in_specs,
        out_specs=out_specs,
        check_vma=False,
    )
```
